512 devices in a mesh: fs: 64 (over z, y), tp: 8 (over x, core).
Axes of the slice: x: 4, y: 8, z: 8, core: 2. Of those that a mesh axis runs over, the one named last changes fastest.
Arguments:
- inputs: bfloat16 [32768, 2048], P('fs', 'tp'), may hold values from -6 to 6
- value_cotangent: bfloat16 [32768, 2048], P('fs', 'tp'), may hold values from -6 to 6
- first_map: bfloat16 [32768, 2048], P('fs', 'tp'), may hold values from -6 to 6
- second_map: bfloat16 [32768, 2048], P('fs', 'tp'), may hold values from -6 to 6
- lambdas: float32 [16], P('tp'), may hold values from 0.3 to 0.8
- head_gain: float32 [128], replicated, may hold values from 0.1 to 1.9
- output_cotangent: bfloat16 [32768, 2048], P('fs', 'tp'), may hold values from -6 to 6
- value_factor: bfloat16 [2048, 256], replicated, may hold values from -0.125 to 0.125
- output_factor: bfloat16 [2048, 256], replicated, may hold values from -0.125 to 0.125
- value_weight: float32 [2048, 2048], P('fs', 'tp'), may hold values from -0.125 to 0.125
- output_weight: float32 [2048, 2048], P('tp', 'fs'), may hold values from -0.125 to 0.125
- value_moment: float32 [256, 2048], P('fs', 'tp'), may hold values from -6 to 6
- value_second: float32 [256, 2048], P('fs', 'tp'), may hold values from 0.25 to 4
- output_moment: float32 [256, 2048], P('fs', 'tp'), may hold values from -6 to 6
- output_second: float32 [256, 2048], P('fs', 'tp'), may hold values from 0.25 to 4
Outputs:
- value_master: float32 [2048, 2048], P('fs', 'tp')
- output_master: float32 [2048, 2048], P('tp', 'fs')
- value_moment_new: float32 [256, 2048], P('fs', 'tp')
- value_second_new: float32 [256, 2048], P('fs', 'tp')
- output_moment_new: float32 [256, 2048], P('fs', 'tp')
- output_second_new: float32 [256, 2048], P('fs', 'tp')
- value_copy: bfloat16 [2048, 2048], P(None, 'tp')
- output_copy: bfloat16 [2048, 2048], P('tp')
The draws below stay inside these ranges and needn't reach their ends.
All inputs are finite; a program needn't handle non-finite values.
Results may differ from the reference program's by a relative error of at most 0.0027.
Values may be sent and summed in bfloat16 or wider, within the bound.
A program may use at most 64 MiB of HBM per device.

```python
import math
import jax
import jax.numpy as jnp
from jax import lax

D = 2048
H = 16
VD = 128
R = 256
TOKENS = 32768


def block_scale(own_key, extent, pieces, smallest, high):
    loudness, own = 1.0, jax.random.fold_in(own_key, 6)
    for dim, blocks in pieces:
        draws = jnp.exp(jax.random.uniform(jax.random.fold_in(own, dim), (blocks,), jnp.float32, smallest / len(pieces), high / len(pieces)))
        loudness = loudness * jnp.repeat(draws, extent[dim] // blocks).reshape([-1 if axis == dim else 1 for axis in range(len(extent))])
    return loudness


def scatter_about(key, extent, spread, limit, shards=(), dtype=jnp.bfloat16):
    values = spread * jax.random.normal(key, extent, jnp.float32)
    if shards:
        values = values * block_scale(key, extent, shards, -0.22, 0.18)
    return jnp.clip(values, -limit, limit).astype(dtype)


def setup_inputs(seed: int = 0) -> dict:
    seeds = jax.random.split(jax.random.key(seed), 16)
    inputs = scatter_about(seeds[0], (TOKENS, D), 1.0, 6.0, ((0, 64), (1, 8)))
    value_cotangent = scatter_about(seeds[1], (TOKENS, H * VD), 1.0, 6.0, ((0, 64), (1, 8)))
    first_map = scatter_about(seeds[2], (TOKENS, H * VD), 1.0, 6.0, ((0, 64), (1, 8)))
    second_map = scatter_about(seeds[3], (TOKENS, H * VD), 1.0, 6.0, ((0, 64), (1, 8)))
    lambdas = jnp.clip(0.3 + 0.5 * jax.random.uniform(seeds[4], (H,), jnp.float32) ** block_scale(seeds[4], (H,), ((0, 8),), -0.2, 0.2), 0.3, 0.8)
    head_gain = jnp.clip(1.0 + 0.18 * jax.random.normal(seeds[5], (VD,), jnp.float32), 0.1, 1.9)
    output_cotangent = scatter_about(seeds[6], (TOKENS, D), 1.0, 6.0, ((0, 64), (1, 8)))
    value_factor = scatter_about(seeds[7], (D, R), D ** -0.5, 0.125)
    output_factor = scatter_about(seeds[8], (D, R), D ** -0.5, 0.125)
    value_weight = scatter_about(seeds[9], (D, H * VD), D ** -0.5, 0.125, ((0, 64), (1, 8)), jnp.float32)
    output_weight = scatter_about(seeds[10], (H * VD, D), (H * VD) ** -0.5, 0.125, ((0, 8), (1, 64)), jnp.float32)
    value_moment = scatter_about(seeds[11], (R, H * VD), 1.0, 6.0, ((0, 64), (1, 8)), jnp.float32)
    value_second = jnp.clip(jnp.exp(math.log(4.0) - 2.7725887 * jax.random.uniform(seeds[12], (R, H * VD), jnp.float32) ** block_scale(seeds[12], (R, H * VD), ((0, 64), (1, 8)), -0.2, 0.2)), 0.25, 4.0)
    output_moment = scatter_about(seeds[13], (R, H * VD), 1.0, 6.0, ((0, 64), (1, 8)), jnp.float32)
    output_second = jnp.clip(jnp.exp(math.log(4.0) - 2.7725887 * jax.random.uniform(seeds[14], (R, H * VD), jnp.float32) ** block_scale(seeds[14], (R, H * VD), ((0, 64), (1, 8)), -0.2, 0.2)), 0.25, 4.0)
    return {"inputs": inputs, "value_cotangent": value_cotangent, "first_map": first_map, "second_map": second_map, "lambdas": lambdas, "head_gain": head_gain, "output_cotangent": output_cotangent, "value_factor": value_factor, "output_factor": output_factor, "value_weight": value_weight, "output_weight": output_weight, "value_moment": value_moment, "value_second": value_second, "output_moment": output_moment, "output_second": output_second}


def contract_rows(left, right, precise):
    if precise:
        return lax.dot_general(left, right, (((0,), (0,)), ((), ())), precision=lax.Precision.HIGHEST, preferred_element_type=jnp.float32)
    return lax.dot_general(left, right, (((0,), (0,)), ((), ())), preferred_element_type=jnp.float32)

def reference(inputs, value_cotangent, first_map, second_map, lambdas, head_gain, output_cotangent, value_factor, output_factor, value_weight, output_weight, value_moment, value_second, output_moment, output_second):
    tok_count = inputs.shape[0]
    first = first_map.astype(jnp.float32).reshape(tok_count, H, VD)
    second = second_map.astype(jnp.float32).reshape(tok_count, H, VD)
    difference = first - lambdas[None, :, None] * second
    normed = difference * lax.rsqrt(lax.optimization_barrier(jnp.mean(difference * difference, axis=-1, keepdims=True)) + 1e-06) * head_gain
    heads_out = normed.reshape(tok_count, H * VD).astype(jnp.bfloat16)
    token_scale = 1.0 / math.sqrt(TOKENS)
    grad_value = contract_rows(inputs, value_cotangent, False) * token_scale
    grad_output_t = contract_rows(output_cotangent, heads_out, False) * token_scale
    low_value = contract_rows(value_factor.astype(jnp.float32), grad_value, True)
    low_output = contract_rows(output_factor.astype(jnp.float32), grad_output_t, True)
    value_moment_new = 0.8 * value_moment + 0.2 * low_value
    value_second_new = 0.95 * value_second + 0.05 * low_value * low_value
    output_moment_new = 0.8 * output_moment + 0.2 * low_output
    output_second_new = 0.95 * output_second + 0.05 * low_output * low_output
    direction_value = value_moment_new / (jnp.sqrt(value_second_new) + 1e-08)
    direction_output = output_moment_new / (jnp.sqrt(output_second_new) + 1e-08)
    step_value = jnp.dot(value_factor.astype(jnp.float32), direction_value, precision=lax.Precision.HIGHEST, preferred_element_type=jnp.float32)
    step_output = jnp.dot(output_factor.astype(jnp.float32), direction_output, precision=lax.Precision.HIGHEST, preferred_element_type=jnp.float32)
    value_master = value_weight - 0.05 * step_value
    output_master = output_weight - 0.05 * step_output.T
    return (value_master, output_master, value_moment_new, value_second_new, output_moment_new, output_second_new, value_master.astype(jnp.bfloat16), output_master.astype(jnp.bfloat16))
```

```python
import functools
import math

import jax
import jax.numpy as jnp
from jax import lax
from jax.experimental import pallas as pl
from jax.experimental.pallas import tpu as pltpu
from jax.sharding import PartitionSpec as P

MESH = pl.DeviceIdType.MESH
X, C, Y, Z = 4, 2, 8, 8
F32, BF16 = jnp.float32, jnp.bfloat16
RANK, HEAD = 256, 128
WIDTH_ROWS = 32
WEIGHT_RATE = 960.0
DIRECTION_RATE = 11.0


def encode(value, rate):
    size = jnp.exp2(jnp.abs(value) * rate) - 1.0
    return jnp.where(value < 0, -size, size).astype(BF16)


def decode(code, rate):
    code = code.astype(F32)
    size = jnp.log(1.0 + jnp.abs(code)) * (1.0 / (rate * math.log(2.0)))
    return jnp.where(code < 0, -size, size)


def rows_dot(left, right):
    return lax.dot_general(left, right, (((0,), (0,)), ((), ())), preferred_element_type=F32)


def exchange_kernel(
    inputs, ocot, vcot, first, second, lambdas, gain, vf, of, vw, ow, vm, vs, om, os_,
    wv_out, wo_out, da_out, db_out, low_out,
    in_v, oc_v, vc_v, fi_v, se_v, vf_v, of_v, vw_v, ow_v, mom_v, sec_v,
    pair, ax, sx, rx, pq, heads,
    la, lb, ra, rb, sa, sb, ra2, rb2, da, db, wv, wo, low_v,
    load_sem, out_sem,
    pair_s, pair_r, xs_s, xs_r, xg_s, xg_r, fw_s, fw_r,
    r1a_s, r1a_r, r1b_s, r1b_r, r2a_s, r2a_r, r2b_s, r2b_r,
    g1a_s, g1a_r, g1b_s, g1b_r, g2a_s, g2a_r, g2b_s, g2b_r,
    w1v_s, w1v_r, w1o_s, w1o_r, wrv_s, wrv_r, wro_s, wro_r,
):
    fs = lax.axis_index("fs")
    tp = lax.axis_index("tp")
    z, y = fs // Y, lax.rem(fs, Y)
    x, c = tp // C, lax.rem(tp, C)

    def at_x(d):
        return (fs, lax.rem(x + d, X) * C + c)

    def at_y(d):
        return (z * Y + lax.rem(y + d, Y), tp)

    def at_z(d):
        return (lax.rem(z + d, Z) * Y + y, tp)

    partner = (fs, x * C + (1 - c))

    def send(src, dst, s, r, where):
        copy = pltpu.make_async_remote_copy(
            src_ref=src, dst_ref=dst, send_sem=s, recv_sem=r, device_id=where, device_id_type=MESH
        )
        copy.start()
        return copy

    chip_rows = pl.ds(pl.multiple_of(x * (C * 256), C * 256), C * 256)
    loads = {}
    for i, (name, src, dst) in enumerate(
        [
            ("vw", vw, vw_v),
            ("ow", ow, ow_v),
            ("in", inputs, in_v),
            ("oc", ocot, oc_v),
            ("vf", vf.at[chip_rows], vf_v),
            ("of", of.at[chip_rows], of_v),
            ("fi", first, fi_v),
            ("se", second, se_v),
            ("vc", vcot, vc_v),
            ("vm", vm, mom_v.at[pl.ds(0, 4)]),
            ("om", om, mom_v.at[pl.ds(4, 4)]),
            ("vs", vs, sec_v.at[pl.ds(0, 4)]),
            ("os", os_, sec_v.at[pl.ds(4, 4)]),
        ]
    ):
        loads[name] = pltpu.make_async_copy(src, dst, load_sem.at[i])
        loads[name].start()

    barrier = pltpu.get_barrier_semaphore()
    friends = (
        [partner]
        + [at_x(d) for d in range(1, X)]
        + [at_y(d) for d in range(1, Y)]
        + [at_z(d) for d in range(1, Z)]
    )
    for friend in friends:
        pl.semaphore_signal(barrier, inc=1, device_id=friend, device_id_type=MESH)

    loads["vw"].wait()
    wv[z, y] = encode(vw_v[...], WEIGHT_RATE)
    loads["ow"].wait()
    turned = jnp.concatenate([ow_v[...], jnp.zeros((256, 128 - WIDTH_ROWS), F32)], axis=1).T
    wo[z, y] = encode(turned[:WIDTH_ROWS], WEIGHT_RATE)
    loads["in"].wait()
    loads["oc"].wait()
    loads["vf"].wait()
    loads["of"].wait()
    pl.semaphore_wait(barrier, len(friends))

    mine = pl.ds(pl.multiple_of(c * 256, 256), 256)
    theirs = pl.ds(pl.multiple_of((1 - c) * 256, 256), 256)
    to_pair = [
        send(in_v.at[theirs], pair.at[0], pair_s.at[0], pair_r.at[0], partner),
        send(oc_v.at[theirs], pair.at[1], pair_s.at[1], pair_r.at[1], partner),
    ]
    w1v = [
        send(wv.at[z, y], wv.at[z, y], w1v_s.at[d], w1v_r.at[d], at_y(d)) for d in range(1, Y)
    ]
    w1o = [
        send(wo.at[z, y], wo.at[z, y], w1o_s.at[d], w1o_r.at[d], at_z(d)) for d in range(1, Z)
    ]
    acc_p = jnp.dot(in_v[mine], vf_v[mine], preferred_element_type=F32)
    acc_q = jnp.dot(oc_v[mine], of_v[mine], preferred_element_type=F32)
    for copy in to_pair:
        copy.wait_recv()
    acc_p += jnp.dot(pair[0], vf_v[theirs], preferred_element_type=F32)
    acc_q += jnp.dot(pair[1], of_v[theirs], preferred_element_type=F32)
    acc = jnp.concatenate([acc_p, acc_q], axis=1).reshape(X, 64, 512)
    ax[...] = acc
    sx[...] = acc.astype(BF16)
    x_sum = [
        send(sx.at[lax.rem(x + d, X)], rx.at[x], xs_s.at[d], xs_r.at[d], at_x(d))
        for d in range(1, X)
    ]

    loads["fi"].wait()
    loads["se"].wait()
    for h in range(2):
        cols = slice(h * HEAD, (h + 1) * HEAD)
        difference = fi_v[:, cols].astype(F32) - lambdas[h] * se_v[:, cols].astype(F32)
        mean = jnp.mean(difference * difference, axis=-1, keepdims=True)
        heads[:, cols] = (difference * lax.rsqrt(mean + 1e-06) * gain[...]).astype(BF16)

    total = ax[x]
    for d, copy in zip(range(1, X), x_sum):
        copy.wait_recv()
        total += rx[lax.rem(x + X - d, X)].astype(F32)
    pq[c, x] = total.astype(BF16)
    x_all = [
        send(pq.at[c, x], pq.at[c, x], xg_s.at[d], xg_r.at[d], at_x(d)) for d in range(1, X)
    ]
    passed = [send(pq.at[c, x], pq.at[c, x], fw_s.at[0], fw_r.at[0], partner)]

    for copy in w1v + w1o:
        copy.wait_recv()

    def ring_step(s):
        out = []
        zr, yr = lax.rem(z + Z - (s - 1), Z), lax.rem(y + Y - (s - 1), Y)
        zl, yl = lax.rem(z + (s - 1), Z), lax.rem(y + (s - 1), Y)
        out.append(send(wv.at[zr], wv.at[zr], wrv_s.at[s], wrv_r.at[s], at_z(1)))
        out.append(
            send(wo.at[:, pl.ds(yr, 1)], wo.at[:, pl.ds(yr, 1)], wro_s.at[s], wro_r.at[s], at_y(1))
        )
        if s < 4:
            k = 4 + s
            out.append(send(wv.at[zl], wv.at[zl], wrv_s.at[k], wrv_r.at[k], at_z(Z - 1)))
            out.append(
                send(
                    wo.at[:, pl.ds(yl, 1)], wo.at[:, pl.ds(yl, 1)], wro_s.at[k], wro_r.at[k],
                    at_y(Y - 1),
                )
            )
        return out

    rings = [ring_step(1)]

    for d, copy in zip(range(1, X), x_all):
        copy.wait_recv()
        xx = lax.rem(x + X - d, X)
        passed.append(send(pq.at[c, xx], pq.at[c, xx], fw_s.at[d], fw_r.at[d], partner))
    loads["vc"].wait()
    pq_mine = pq[c].reshape(256, 512)
    lv = rows_dot(pq_mine[:, :RANK], vc_v[mine])
    lo = rows_dot(pq_mine[:, RANK:], heads[mine])
    for copy in passed:
        copy.wait_recv()
    pq_theirs = pq[1 - c].reshape(256, 512)
    lv += rows_dot(pq_theirs[:, :RANK], vc_v[theirs])
    lo += rows_dot(pq_theirs[:, RANK:], heads[theirs])
    scale = 1.0 / math.sqrt(32768.0)
    lv3 = (lv * scale).reshape(32, 8, 256)
    lo3 = (lo * scale).reshape(32, 8, 256)
    upper = lax.broadcasted_iota(jnp.int32, (32, 8, 256), 1) < 4
    even = jnp.where(upper, lv3, pltpu.roll(lo3, 4, 1)).astype(BF16)
    odd = jnp.where(upper, pltpu.roll(lv3, 4, 1), lo3).astype(BF16)
    for f in range(Z * Y):
        block = (odd if f % 2 else even)[f // 2]
        la[f // Y, f % Y] = block[:, :128]
        lb[f % Y, f // Y] = block[:, 128:]
    r1a = [
        send(la.at[lax.rem(z + d, Z)], ra.at[z], r1a_s.at[d], r1a_r.at[d], at_z(d))
        for d in range(1, Z)
    ]
    r1b = [
        send(lb.at[lax.rem(y + d, Y)], rb.at[y], r1b_s.at[d], r1b_r.at[d], at_y(d))
        for d in range(1, Y)
    ]

    for copy in rings[0]:
        copy.wait_recv()
    rings.append(ring_step(2))

    sum_a = la[z].astype(F32)
    sum_b = lb[y].astype(F32)
    for d in range(1, 8):
        r1a[d - 1].wait_recv()
        sum_a += ra[lax.rem(z + Z - d, Z)].astype(F32)
        r1b[d - 1].wait_recv()
        sum_b += rb[lax.rem(y + Y - d, Y)].astype(F32)
    sa[...] = sum_a
    sb[...] = sum_b
    r2a = [
        send(sa.at[lax.rem(y + d, Y)], ra2.at[y], r2a_s.at[d], r2a_r.at[d], at_y(d))
        for d in range(1, Y)
    ]
    r2b = [
        send(sb.at[lax.rem(z + d, Z)], rb2.at[z], r2b_s.at[d], r2b_r.at[d], at_z(d))
        for d in range(1, Z)
    ]

    for copy in rings[1]:
        copy.wait_recv()
    rings.append(ring_step(3))

    low_a = sa[y]
    low_b = sb[z]
    for d in range(1, 8):
        r2a[d - 1].wait_recv()
        low_a += ra2[lax.rem(y + Y - d, Y)]
        r2b[d - 1].wait_recv()
        low_b += rb2[lax.rem(z + Z - d, Z)]
    low = jnp.concatenate([low_a, low_b], axis=1)
    low_v[...] = low
    for name in ("vm", "om", "vs", "os"):
        loads[name].wait()
    moment = 0.8 * mom_v[...] + 0.2 * low
    spread = 0.95 * sec_v[...] + 0.05 * low * low
    code = encode(moment / (jnp.sqrt(spread) + 1e-08), DIRECTION_RATE)
    da[z, y] = code[:, :128]
    db[y, z] = code[:, 128:]
    g1a = [
        send(da.at[z, y], da.at[z, y], g1a_s.at[d], g1a_r.at[d], at_y(d)) for d in range(1, Y)
    ]
    g1b = [
        send(db.at[y, z], db.at[y, z], g1b_s.at[d], g1b_r.at[d], at_z(d)) for d in range(1, Z)
    ]

    for copy in rings[2]:
        copy.wait_recv()
    rings.append(ring_step(4))

    for copy in g1a:
        copy.wait_recv()
    g2a = [send(da.at[z], da.at[z], g2a_s.at[d], g2a_r.at[d], at_z(d)) for d in range(1, Z)]
    for copy in g1b:
        copy.wait_recv()
    g2b = [send(db.at[y], db.at[y], g2b_s.at[d], g2b_r.at[d], at_y(d)) for d in range(1, Y)]

    for copy in rings[3]:
        copy.wait_recv()
    outs = [
        pltpu.make_async_copy(wv, wv_out, out_sem.at[0]),
        pltpu.make_async_copy(wo, wo_out, out_sem.at[1]),
        pltpu.make_async_copy(low_v, low_out, out_sem.at[2]),
    ]
    for copy in outs:
        copy.start()
    for copy in g2a + g2b:
        copy.wait_recv()
    last = [
        pltpu.make_async_copy(da, da_out, out_sem.at[3]),
        pltpu.make_async_copy(db, db_out, out_sem.at[4]),
    ]
    for copy in last:
        copy.start()
    sent = to_pair + w1v + w1o + x_sum + x_all + passed + r1a + r1b + r2a + r2b
    sent += g1a + g1b + g2a + g2b
    for ring in rings:
        sent += ring
    for copy in sent:
        copy.wait_send()
    for copy in outs + last:
        copy.wait()


def finish_kernel(
    da, db, wv, wo, vf, of, low, vw, ow, vm, vs, om, os_,
    vmaster, omaster, vm_new, vs_new, om_new, os_new, vcopy, ocopy,
    dv_hi, dv_lo, do_hi, do_lo, sv, so, turn,
):
    j = pl.program_id(0)
    fs = lax.axis_index("fs")

    @pl.when(j == 0)
    def _():
        low_v, low_o = low[0:4], low[4:8]
        vm_new[...] = 0.8 * vm[...] + 0.2 * low_v
        vs_new[...] = 0.95 * vs[...] + 0.05 * low_v * low_v
        om_new[...] = 0.8 * om[...] + 0.2 * low_o
        os_new[...] = 0.95 * os_[...] + 0.05 * low_o * low_o
        upper = lax.broadcasted_iota(jnp.int32, (8, 256), 0) < 4
        for g in range(Z * Y // 2):
            zz, yy = (2 * g) // Y, (2 * g) % Y
            even = decode(jnp.concatenate([da[zz, yy], db[yy, zz]], axis=1), DIRECTION_RATE)
            odd = decode(
                jnp.concatenate([da[zz, yy + 1], db[yy + 1, zz]], axis=1), DIRECTION_RATE
            )
            value = jnp.where(upper, even, pltpu.roll(odd, 4, 0))
            output = jnp.where(upper, pltpu.roll(even, 4, 0), odd)
            rows = slice(8 * g, 8 * g + 8)
            for full, hi, lo in ((value, dv_hi, dv_lo), (output, do_hi, do_lo)):
                top = full.astype(BF16)
                hi[rows] = top
                lo[rows] = (full - top.astype(F32)).astype(BF16)

    def step(factor, hi, lo):
        out = jnp.dot(factor[...], hi[...], preferred_element_type=F32)
        return 0.05 * (out + jnp.dot(factor[...], lo[...], preferred_element_type=F32))

    sv[...] = step(vf, dv_hi, dv_lo)
    so[...] = step(of, do_hi, do_lo)
    vcopy[...] = (decode(wv[...], WEIGHT_RATE) - sv[...]).astype(BF16)
    ocopy[...] = (decode(wo[...], WEIGHT_RATE) - so[...]).T.astype(BF16)

    @pl.when(j == fs // 8)
    def _():
        rows = pl.ds(pl.multiple_of(lax.rem(fs, 8) * WIDTH_ROWS, WIDTH_ROWS), WIDTH_ROWS)
        vmaster[...] = vw[...] - sv[rows]
        turn[0:WIDTH_ROWS] = so[rows]
        omaster[...] = ow[...] - turn[...].T[:, :WIDTH_ROWS]


def local(
    inputs, value_cotangent, first_map, second_map, lambdas, head_gain, output_cotangent,
    value_factor, output_factor, value_weight, output_weight,
    value_moment, value_second, output_moment, output_second,
):
    gain = head_gain.reshape(1, HEAD)
    any_spec = pl.BlockSpec(memory_space=pl.ANY)
    dma = pltpu.SemaphoreType.DMA
    vmem = pltpu.VMEM
    sems = [dma((13,)), dma((5,)), dma((2,)), dma((2,)), dma((4,)), dma((4,)), dma((4,)), dma((4,)), dma((4,)), dma((4,))]
    sems += [dma((8,))] * 24
    wv, wo, da, db, low = pl.pallas_call(
        exchange_kernel,
        out_shape=[
            jax.ShapeDtypeStruct((Z, Y, WIDTH_ROWS, 256), BF16),
            jax.ShapeDtypeStruct((Z, Y, WIDTH_ROWS, 256), BF16),
            jax.ShapeDtypeStruct((Z, Y, 8, 128), BF16),
            jax.ShapeDtypeStruct((Y, Z, 8, 128), BF16),
            jax.ShapeDtypeStruct((8, 256), F32),
        ],
        in_specs=[any_spec] * 5
        + [pl.BlockSpec(memory_space=pltpu.SMEM), pl.BlockSpec(memory_space=pltpu.VMEM)]
        + [any_spec] * 8,
        out_specs=[any_spec] * 5,
        scratch_shapes=[
            vmem((512, 256), BF16), vmem((512, 256), BF16), vmem((512, 256), BF16),
            vmem((512, 256), BF16), vmem((512, 256), BF16),
            vmem((512, 256), BF16), vmem((512, 256), BF16),
            vmem((WIDTH_ROWS, 256), F32), vmem((256, WIDTH_ROWS), F32),
            vmem((8, 256), F32), vmem((8, 256), F32),
            vmem((2, 256, 256), BF16), vmem((X, 64, 512), F32), vmem((X, 64, 512), BF16),
            vmem((X, 64, 512), BF16), vmem((C, X, 64, 512), BF16), vmem((512, 256), BF16),
            vmem((Z, Y, 8, 128), BF16), vmem((Y, Z, 8, 128), BF16),
            vmem((Z, Y, 8, 128), BF16), vmem((Y, Z, 8, 128), BF16),
            vmem((Y, 8, 128), F32), vmem((Z, 8, 128), F32),
            vmem((Y, 8, 128), F32), vmem((Z, 8, 128), F32),
            vmem((Z, Y, 8, 128), BF16), vmem((Y, Z, 8, 128), BF16),
            vmem((Z, Y, WIDTH_ROWS, 256), BF16), vmem((Z, Y, WIDTH_ROWS, 256), BF16),
            vmem((8, 256), F32),
        ]
        + sems,
        compiler_params=pltpu.CompilerParams(
            collective_id=0, has_side_effects=True, vmem_limit_bytes=24 * 1024 * 1024
        ),
        name="exchange",
    )(
        inputs, output_cotangent, value_cotangent, first_map, second_map, lambdas, gain,
        value_factor, output_factor, value_weight, output_weight,
        value_moment, value_second, output_moment, output_second,
    )
    width, cols = 2048, 256
    wv, wo = wv.reshape(width, cols), wo.reshape(width, cols)

    def whole(shape):
        return pl.BlockSpec(shape, lambda j: (0,) * len(shape))

    rows = pl.BlockSpec((256, cols), lambda j: (j, 0))
    return pl.pallas_call(
        finish_kernel,
        grid=(width // 256,),
        out_shape=[
            jax.ShapeDtypeStruct((WIDTH_ROWS, cols), F32),
            jax.ShapeDtypeStruct((cols, WIDTH_ROWS), F32),
            jax.ShapeDtypeStruct((4, cols), F32),
            jax.ShapeDtypeStruct((4, cols), F32),
            jax.ShapeDtypeStruct((4, cols), F32),
            jax.ShapeDtypeStruct((4, cols), F32),
            jax.ShapeDtypeStruct((width, cols), BF16),
            jax.ShapeDtypeStruct((cols, width), BF16),
        ],
        in_specs=[
            whole((Z, Y, 8, 128)), whole((Y, Z, 8, 128)), rows, rows, rows, rows,
            whole((8, cols)), whole((WIDTH_ROWS, cols)), whole((cols, WIDTH_ROWS)),
            whole((4, cols)), whole((4, cols)), whole((4, cols)), whole((4, cols)),
        ],
        out_specs=[
            whole((WIDTH_ROWS, cols)), whole((cols, WIDTH_ROWS)),
            whole((4, cols)), whole((4, cols)), whole((4, cols)), whole((4, cols)),
            rows, pl.BlockSpec((cols, 256), lambda j: (0, j)),
        ],
        scratch_shapes=[vmem((RANK, cols), BF16)] * 4
        + [vmem((256, cols), F32)] * 2
        + [vmem((128, cols), F32)],
        name="finish",
    )(
        da, db, wv, wo, value_factor, output_factor, low, value_weight, output_weight,
        value_moment, value_second, output_moment, output_second,
    )


def solution(mesh):
    both = P("fs", "tp")
    in_specs = (
        both, both, both, both, P("tp"), P(), both, P(), P(), both, P("tp", "fs"),
        both, both, both, both,
    )
    out_specs = (
        both, P("tp", "fs"), both, both, both, both, P(None, "tp"), P("tp", None),
    )
    return jax.shard_map(local, mesh=mesh, in_specs=in_specs, out_specs=out_specs, check_vma=False)
```

```python
import functools
import math

import jax
import jax.numpy as jnp
from jax import lax
from jax.experimental import pallas as pl
from jax.experimental.pallas import tpu as pltpu
from jax.sharding import PartitionSpec as P

MESH = pl.DeviceIdType.MESH
X, C, Y, Z = 4, 2, 8, 8
F32, BF16 = jnp.float32, jnp.bfloat16
RANK, HEAD = 256, 128
FAR = (4, 3, 5, 2, 6, 1, 7)
NEAR = (1, 7, 2, 6, 3, 5, 4)
WIDTH_ROWS = 32
STEP = 512
WEIGHT_RATE = 960.0
DIRECTION_RATE = 11.0


def encode(value, rate):
    size = jnp.exp2(jnp.abs(value) * rate) - 1.0
    return jnp.where(value < 0, -size, size).astype(BF16)


def decode(code, rate):
    code = code.astype(F32)
    size = jnp.log(1.0 + jnp.abs(code)) * (1.0 / (rate * math.log(2.0)))
    return jnp.where(code < 0, -size, size)


def rows_dot(left, right):
    return lax.dot_general(left, right, (((0,), (0,)), ((), ())), preferred_element_type=F32)


def exchange_kernel(
    inputs, ocot, vcot, first, second, lambdas, gain, vf, of, vw, ow, vm, vs, om, os_,
    wv_out, wo_out, da_out, db_out, low_out,
    in_v, oc_v, vc_v, fi_v, se_v, vf_v, of_v, vw_v, ow_v, mom_v, sec_v,
    pair, ax, sx, rx, pq, heads,
    la, lb, ra, rb, sa, sb, ra2, rb2, da, db, wv, wo, low_v, wv_f, wo_f,
    load_sem, out_sem,
    pair_s, pair_r, xs_s, xs_r, xg_s, xg_r, fw_s, fw_r,
    r1a_s, r1a_r, r1b_s, r1b_r, r2a_s, r2a_r, r2b_s, r2b_r,
    g1a_s, g1a_r, g1b_s, g1b_r, g2a_s, g2a_r, g2b_s, g2b_r,
    w1v_s, w1v_r, w1o_s, w1o_r, wrv_s, wrv_r, wro_s, wro_r,
):
    fs = lax.axis_index("fs")
    tp = lax.axis_index("tp")
    z, y = fs // Y, lax.rem(fs, Y)
    x, c = tp // C, lax.rem(tp, C)

    def at_x(d):
        return (fs, lax.rem(x + d, X) * C + c)

    def at_y(d):
        return (z * Y + lax.rem(y + d, Y), tp)

    def at_z(d):
        return (lax.rem(z + d, Z) * Y + y, tp)

    partner = (fs, x * C + (1 - c))

    def send(src, dst, s, r, where):
        copy = pltpu.make_async_remote_copy(
            src_ref=src, dst_ref=dst, send_sem=s, recv_sem=r, device_id=where, device_id_type=MESH
        )
        copy.start()
        return copy

    chip_rows = pl.ds(pl.multiple_of(x * (C * 256), C * 256), C * 256)
    loads = {}
    for i, (name, src, dst) in enumerate(
        [
            ("vw", vw, vw_v),
            ("ow", ow, ow_v),
            ("in", inputs, in_v),
            ("oc", ocot, oc_v),
            ("vf", vf.at[chip_rows], vf_v),
            ("of", of.at[chip_rows], of_v),
            ("fi", first, fi_v),
            ("se", second, se_v),
            ("vc", vcot, vc_v),
            ("vm", vm, mom_v.at[pl.ds(0, 4)]),
            ("om", om, mom_v.at[pl.ds(4, 4)]),
            ("vs", vs, sec_v.at[pl.ds(0, 4)]),
            ("os", os_, sec_v.at[pl.ds(4, 4)]),
        ]
    ):
        loads[name] = pltpu.make_async_copy(src, dst, load_sem.at[i])
        loads[name].start()

    barrier = pltpu.get_barrier_semaphore()
    friends = (
        [partner]
        + [at_x(d) for d in range(1, X)]
        + [at_y(d) for d in range(1, Y)]
        + [at_z(d) for d in range(1, Z)]
    )
    for friend in friends:
        pl.semaphore_signal(barrier, inc=1, device_id=friend, device_id_type=MESH)

    loads["vw"].wait()
    wv[z, y] = encode(vw_v[...], WEIGHT_RATE)
    loads["ow"].wait()
    wo[z, y] = encode(ow_v[...], WEIGHT_RATE)
    loads["in"].wait()
    loads["oc"].wait()
    loads["vf"].wait()
    loads["of"].wait()
    pl.semaphore_wait(barrier, len(friends))

    mine = pl.ds(pl.multiple_of(c * 256, 256), 256)
    theirs = pl.ds(pl.multiple_of((1 - c) * 256, 256), 256)
    to_pair = [
        send(in_v.at[theirs], pair.at[0], pair_s.at[0], pair_r.at[0], partner),
        send(oc_v.at[theirs], pair.at[1], pair_s.at[1], pair_r.at[1], partner),
    ]
    w1v = {
        d: send(wv.at[z, y], wv.at[z, y], w1v_s.at[d], w1v_r.at[d], at_y(d)) for d in FAR
    }
    w1o = {
        d: send(wo.at[z, y], wo.at[z, y], w1o_s.at[d], w1o_r.at[d], at_z(d)) for d in FAR
    }
    acc_p = jnp.dot(in_v[mine], vf_v[mine], preferred_element_type=F32)
    acc_q = jnp.dot(oc_v[mine], of_v[mine], preferred_element_type=F32)
    for copy in to_pair:
        copy.wait_recv()
    acc_p += jnp.dot(pair[0], vf_v[theirs], preferred_element_type=F32)
    acc_q += jnp.dot(pair[1], of_v[theirs], preferred_element_type=F32)
    acc = jnp.concatenate([acc_p, acc_q], axis=1).reshape(X, 64, 512)
    ax[...] = acc
    sx[...] = acc.astype(BF16)
    x_sum = {
        d: send(sx.at[lax.rem(x + d, X)], rx.at[x], xs_s.at[d], xs_r.at[d], at_x(d))
        for d in (2, 1, 3)
    }

    def ring_step(s):
        zr, yr = lax.rem(z + Z - (s - 1), Z), lax.rem(y + Y - (s - 1), Y)
        zl, yl = lax.rem(z + (s - 1), Z), lax.rem(y + (s - 1), Y)
        first_half = pl.ds(0, 8 if s < 4 else 4)
        other_half = pl.ds(0, 8) if s < 4 else pl.ds(4, 4)
        moves = [
            (wv.at[zr, first_half], wrv_s, wrv_r, s, at_z(1)),
            (wo.at[first_half, pl.ds(yr, 1)], wro_s, wro_r, s, at_y(1)),
            (wv.at[zl, other_half], wrv_s, wrv_r, 4 + s, at_z(Z - 1)),
            (wo.at[other_half, pl.ds(yl, 1)], wro_s, wro_r, 4 + s, at_y(Y - 1)),
        ]
        return [send(ref, ref, ss.at[k], rs.at[k], where) for ref, ss, rs, k, where in moves]

    def open_group(at):
        wv_f[at] = decode(wv[at].reshape(256, 256), WEIGHT_RATE)

    for d in NEAR:
        w1v[d].wait_recv()
        w1o[d].wait_recv()
    rings = [ring_step(1)]

    loads["fi"].wait()
    loads["se"].wait()
    for h in range(2):
        cols = slice(h * HEAD, (h + 1) * HEAD)
        difference = fi_v[:, cols].astype(F32) - lambdas[h] * se_v[:, cols].astype(F32)
        mean = jnp.mean(difference * difference, axis=-1, keepdims=True)
        heads[:, cols] = (difference * lax.rsqrt(mean + 1e-06) * gain[...]).astype(BF16)

    total = ax[x]
    for d in (1, 3, 2):
        x_sum[d].wait_recv()
        total += rx[lax.rem(x + X - d, X)].astype(F32)
    pq[c, x] = total.astype(BF16)
    x_all = {
        d: send(pq.at[c, x], pq.at[c, x], xg_s.at[d], xg_r.at[d], at_x(d)) for d in (2, 1, 3)
    }
    passed = [send(pq.at[c, x], pq.at[c, x], fw_s.at[0], fw_r.at[0], partner)]

    for copy in rings[0]:
        copy.wait_recv()
    rings.append(ring_step(2))
    open_group(z)
    open_group(lax.rem(z + Z - 1, Z))
    open_group(lax.rem(z + 1, Z))

    for d in (1, 3, 2):
        x_all[d].wait_recv()
        xx = lax.rem(x + X - d, X)
        passed.append(send(pq.at[c, xx], pq.at[c, xx], fw_s.at[d], fw_r.at[d], partner))
    loads["vc"].wait()
    pq_mine = pq[c].reshape(256, 512)
    lv = rows_dot(pq_mine[:, :RANK], vc_v[mine])
    lo = rows_dot(pq_mine[:, RANK:], heads[mine])
    for copy in rings[1]:
        copy.wait_recv()
    rings.append(ring_step(3))
    for copy in passed:
        copy.wait_recv()
    pq_theirs = pq[1 - c].reshape(256, 512)
    lv += rows_dot(pq_theirs[:, :RANK], vc_v[theirs])
    lo += rows_dot(pq_theirs[:, RANK:], heads[theirs])
    scale = 1.0 / math.sqrt(32768.0)
    lv3 = (lv * scale).reshape(32, 8, 256)
    lo3 = (lo * scale).reshape(32, 8, 256)
    upper = lax.broadcasted_iota(jnp.int32, (32, 8, 256), 1) < 4
    even = jnp.where(upper, lv3, pltpu.roll(lo3, 4, 1)).astype(BF16)
    odd = jnp.where(upper, pltpu.roll(lv3, 4, 1), lo3).astype(BF16)
    for f in range(Z * Y):
        block = (odd if f % 2 else even)[f // 2]
        la[f // Y, f % Y] = block[:, :128]
        lb[f % Y, f // Y] = block[:, 128:]
    r1a, r1b = {}, {}
    for d in FAR:
        r1a[d] = send(la.at[lax.rem(z + d, Z)], ra.at[z], r1a_s.at[d], r1a_r.at[d], at_z(d))
        r1b[d] = send(lb.at[lax.rem(y + d, Y)], rb.at[y], r1b_s.at[d], r1b_r.at[d], at_y(d))

    open_group(lax.rem(z + Z - 2, Z))
    open_group(lax.rem(z + 2, Z))
    for copy in rings[2]:
        copy.wait_recv()
    rings.append(ring_step(4))
    open_group(lax.rem(z + Z - 3, Z))
    open_group(lax.rem(z + 3, Z))

    sum_a = la[z].astype(F32)
    sum_b = lb[y].astype(F32)
    for d in NEAR:
        r1a[d].wait_recv()
        sum_a += ra[lax.rem(z + Z - d, Z)].astype(F32)
        r1b[d].wait_recv()
        sum_b += rb[lax.rem(y + Y - d, Y)].astype(F32)
    sa[...] = sum_a
    sb[...] = sum_b
    r2a, r2b = {}, {}
    for d in FAR:
        r2a[d] = send(sa.at[lax.rem(y + d, Y)], ra2.at[y], r2a_s.at[d], r2a_r.at[d], at_y(d))
        r2b[d] = send(sb.at[lax.rem(z + d, Z)], rb2.at[z], r2b_s.at[d], r2b_r.at[d], at_z(d))

    for copy in rings[3]:
        copy.wait_recv()
    open_group(lax.rem(z + 4, Z))
    for k in range(Z // 2):
        wo_f[:, k * 256 : (k + 1) * 256] = decode(wo[k].reshape(256, 256).T, WEIGHT_RATE)

    low_a = sa[y]
    low_b = sb[z]
    for d in NEAR:
        r2a[d].wait_recv()
        low_a += ra2[lax.rem(y + Y - d, Y)]
        r2b[d].wait_recv()
        low_b += rb2[lax.rem(z + Z - d, Z)]
    low = jnp.concatenate([low_a, low_b], axis=1)
    low_v[...] = low
    for name in ("vm", "om", "vs", "os"):
        loads[name].wait()
    moment = 0.8 * mom_v[...] + 0.2 * low
    spread = 0.95 * sec_v[...] + 0.05 * low * low
    code = encode(moment / (jnp.sqrt(spread) + 1e-08), DIRECTION_RATE)
    da[z, y] = code[:, :128]
    db[y, z] = code[:, 128:]
    g1a, g1b, g2a, g2b = {}, {}, {}, {}
    for d in FAR:
        g1a[d] = send(da.at[z, y], da.at[z, y], g1a_s.at[d], g1a_r.at[d], at_y(d))
        g1b[d] = send(db.at[y, z], db.at[y, z], g1b_s.at[d], g1b_r.at[d], at_z(d))

    for k in range(Z // 2, Z):
        wo_f[:, k * 256 : (k + 1) * 256] = decode(wo[k].reshape(256, 256).T, WEIGHT_RATE)
    outs = [
        pltpu.make_async_copy(wv_f, wv_out, out_sem.at[0]),
        pltpu.make_async_copy(wo_f, wo_out, out_sem.at[1]),
        pltpu.make_async_copy(low_v, low_out, out_sem.at[2]),
    ]
    for copy in outs:
        copy.start()

    for d in NEAR:
        g1a[d].wait_recv()
    for d in FAR:
        g2a[d] = send(da.at[z], da.at[z], g2a_s.at[d], g2a_r.at[d], at_z(d))
    for d in NEAR:
        g1b[d].wait_recv()
    for d in FAR:
        g2b[d] = send(db.at[y], db.at[y], g2b_s.at[d], g2b_r.at[d], at_y(d))
    for d in NEAR:
        g2a[d].wait_recv()
        g2b[d].wait_recv()
    last = [
        pltpu.make_async_copy(da, da_out, out_sem.at[3]),
        pltpu.make_async_copy(db, db_out, out_sem.at[4]),
    ]
    for copy in last:
        copy.start()
    sent = to_pair + passed
    for group in (w1v, w1o, x_sum, x_all, r1a, r1b, r2a, r2b, g1a, g1b, g2a, g2b):
        sent += list(group.values())
    for ring in rings:
        sent += ring
    for copy in sent:
        copy.wait_send()
    for copy in outs + last:
        copy.wait()


def finish_kernel(
    da, db, wv, wo, vf, of, low, vw, ow, vm, vs, om, os_,
    vmaster, omaster, vm_new, vs_new, om_new, os_new, vcopy, ocopy,
    dv, do, do_t,
):
    j = pl.program_id(0)
    fs = lax.axis_index("fs")

    @pl.when(j == 0)
    def _():
        low_v, low_o = low[0:4], low[4:8]
        vm_new[...] = 0.8 * vm[...] + 0.2 * low_v
        vs_new[...] = 0.95 * vs[...] + 0.05 * low_v * low_v
        om_new[...] = 0.8 * om[...] + 0.2 * low_o
        os_new[...] = 0.95 * os_[...] + 0.05 * low_o * low_o
        upper = lax.broadcasted_iota(jnp.int32, (8, 256), 0) < 4
        for g in range(Z * Y // 2):
            zz, yy = (2 * g) // Y, (2 * g) % Y
            even = jnp.concatenate([da[zz, yy], db[yy, zz]], axis=1)
            odd = jnp.concatenate([da[zz, yy + 1], db[yy + 1, zz]], axis=1)
            even = 0.05 * decode(even, DIRECTION_RATE)
            odd = 0.05 * decode(odd, DIRECTION_RATE)
            value = jnp.where(upper, even, pltpu.roll(odd, 4, 0))
            output = jnp.where(upper, pltpu.roll(even, 4, 0), odd)
            for full, both in ((value, dv), (output, do)):
                top = full.astype(BF16)
                both[8 * g : 8 * g + 8] = top
                both[RANK + 8 * g : RANK + 8 * g + 8] = (full - top.astype(F32)).astype(BF16)
        do_t[...] = do[...].T

    factor_v = vf[...]
    step_v = jnp.dot(
        jnp.concatenate([factor_v, factor_v], axis=1), dv[...], preferred_element_type=F32
    )
    vcopy[...] = (wv[...] - step_v).astype(BF16)
    factor_o = of[...]
    step_o = lax.dot_general(
        do_t[...],
        jnp.concatenate([factor_o, factor_o], axis=1),
        (((1,), (1,)), ((), ())),
        preferred_element_type=F32,
    )
    ocopy[...] = (wo[...] - step_o).astype(BF16)

    @pl.when(j == fs // (STEP // WIDTH_ROWS))
    def _():
        at = lax.rem(fs, STEP // WIDTH_ROWS) * WIDTH_ROWS
        rows = pl.ds(pl.multiple_of(at, WIDTH_ROWS), WIDTH_ROWS)
        for factor, both, weight, out in ((vf, dv, vw, vmaster), (of, do, ow, omaster)):
            own = factor[rows]
            out[...] = weight[...] - jnp.dot(
                jnp.concatenate([own, own], axis=1), both[...], preferred_element_type=F32
            )


def local(
    inputs, value_cotangent, first_map, second_map, lambdas, head_gain, output_cotangent,
    value_factor, output_factor, value_weight, output_weight,
    value_moment, value_second, output_moment, output_second,
):
    turned_weight = output_weight.T
    gain = head_gain.reshape(1, HEAD)
    any_spec = pl.BlockSpec(memory_space=pl.ANY)
    dma = pltpu.SemaphoreType.DMA
    vmem = pltpu.VMEM
    sems = [dma((13,)), dma((5,)), dma((2,)), dma((2,)), dma((4,)), dma((4,)), dma((4,)), dma((4,)), dma((4,)), dma((4,))]
    sems += [dma((8,))] * 20 + [dma((9,))] * 4
    wv, wo, da, db, low = pl.pallas_call(
        exchange_kernel,
        out_shape=[
            jax.ShapeDtypeStruct((Z, 256, 256), F32),
            jax.ShapeDtypeStruct((256, 2048), F32),
            jax.ShapeDtypeStruct((Z, Y, 8, 128), BF16),
            jax.ShapeDtypeStruct((Y, Z, 8, 128), BF16),
            jax.ShapeDtypeStruct((8, 256), F32),
        ],
        in_specs=[any_spec] * 5
        + [pl.BlockSpec(memory_space=pltpu.SMEM), pl.BlockSpec(memory_space=pltpu.VMEM)]
        + [any_spec] * 8,
        out_specs=[any_spec] * 5,
        scratch_shapes=[
            vmem((512, 256), BF16), vmem((512, 256), BF16), vmem((512, 256), BF16),
            vmem((512, 256), BF16), vmem((512, 256), BF16),
            vmem((512, 256), BF16), vmem((512, 256), BF16),
            vmem((WIDTH_ROWS, 256), F32), vmem((WIDTH_ROWS, 256), F32),
            vmem((8, 256), F32), vmem((8, 256), F32),
            vmem((2, 256, 256), BF16), vmem((X, 64, 512), F32), vmem((X, 64, 512), BF16),
            vmem((X, 64, 512), BF16), vmem((C, X, 64, 512), BF16), vmem((512, 256), BF16),
            vmem((Z, Y, 8, 128), BF16), vmem((Y, Z, 8, 128), BF16),
            vmem((Z, Y, 8, 128), BF16), vmem((Y, Z, 8, 128), BF16),
            vmem((Y, 8, 128), F32), vmem((Z, 8, 128), F32),
            vmem((Y, 8, 128), F32), vmem((Z, 8, 128), F32),
            vmem((Z, Y, 8, 128), BF16), vmem((Y, Z, 8, 128), BF16),
            vmem((Z, Y, WIDTH_ROWS, 256), BF16), vmem((Z, Y, WIDTH_ROWS, 256), BF16),
            vmem((8, 256), F32), vmem((Z, 256, 256), F32), vmem((256, 2048), F32),
        ]
        + sems,
        compiler_params=pltpu.CompilerParams(
            collective_id=0, has_side_effects=True, vmem_limit_bytes=60 * 1024 * 1024
        ),
        name="exchange",
    )(
        inputs, output_cotangent, value_cotangent, first_map, second_map, lambdas, gain,
        value_factor, output_factor, value_weight, turned_weight,
        value_moment, value_second, output_moment, output_second,
    )
    width, cols = 2048, 256
    wv = wv.reshape(width, cols)

    def whole(shape):
        return pl.BlockSpec(shape, lambda j: (0,) * len(shape))

    rows = pl.BlockSpec((STEP, cols), lambda j: (j, 0))
    turned = pl.BlockSpec((cols, STEP), lambda j: (0, j))
    vmaster, omaster, *rest = pl.pallas_call(
        finish_kernel,
        grid=(width // STEP,),
        out_shape=[
            jax.ShapeDtypeStruct((WIDTH_ROWS, cols), F32),
            jax.ShapeDtypeStruct((WIDTH_ROWS, cols), F32),
            jax.ShapeDtypeStruct((4, cols), F32),
            jax.ShapeDtypeStruct((4, cols), F32),
            jax.ShapeDtypeStruct((4, cols), F32),
            jax.ShapeDtypeStruct((4, cols), F32),
            jax.ShapeDtypeStruct((width, cols), BF16),
            jax.ShapeDtypeStruct((cols, width), BF16),
        ],
        in_specs=[
            whole((Z, Y, 8, 128)), whole((Y, Z, 8, 128)), rows, turned, rows, rows,
            whole((8, cols)), whole((WIDTH_ROWS, cols)), whole((WIDTH_ROWS, cols)),
            whole((4, cols)), whole((4, cols)), whole((4, cols)), whole((4, cols)),
        ],
        out_specs=[
            whole((WIDTH_ROWS, cols)), whole((WIDTH_ROWS, cols)),
            whole((4, cols)), whole((4, cols)), whole((4, cols)), whole((4, cols)),
            rows, turned,
        ],
        scratch_shapes=[
            vmem((2 * RANK, cols), BF16), vmem((2 * RANK, cols), BF16), vmem((cols, 2 * RANK), BF16),
        ],
        compiler_params=pltpu.CompilerParams(vmem_limit_bytes=60 * 1024 * 1024),
        name="finish",
    )(
        da, db, wv, wo, value_factor, output_factor, low, value_weight, turned_weight,
        value_moment, value_second, output_moment, output_second,
    )
    return (vmaster, omaster.T, *rest)


def solution(mesh):
    both = P("fs", "tp")
    in_specs = (
        both, both, both, both, P("tp"), P(), both, P(), P(), both, P("tp", "fs"),
        both, both, both, both,
    )
    out_specs = (
        both, P("tp", "fs"), both, both, both, both, P(None, "tp"), P("tp", None),
    )
    return jax.shard_map(local, mesh=mesh, in_specs=in_specs, out_specs=out_specs, check_vma=False)
```

```python
import functools
import math

import jax
import jax.numpy as jnp
from jax import lax
from jax.experimental import pallas as pl
from jax.experimental.pallas import tpu as pltpu
from jax.sharding import PartitionSpec as P

MESH = pl.DeviceIdType.MESH
X, C, Y, Z = 4, 2, 8, 8
F32, BF16 = jnp.float32, jnp.bfloat16
RANK, HEAD = 256, 128
FAR = (4, 3, 5, 2, 6, 1, 7)
NEAR = (1, 7, 2, 6, 3, 5, 4)
WIDTH_ROWS = 32
STEP = 512
CHUNKS = 2048 // STEP
WEIGHT_RATE = 960.0
DIRECTION_RATE = 11.0


def encode(value, rate):
    size = jnp.exp2(jnp.abs(value) * rate) - 1.0
    return jnp.where(value < 0, -size, size).astype(BF16)


def decode(code, rate):
    code = code.astype(F32)
    size = jnp.log(1.0 + jnp.abs(code)) * (1.0 / (rate * math.log(2.0)))
    return jnp.where(code < 0, -size, size)


def rows_dot(left, right):
    return lax.dot_general(left, right, (((0,), (0,)), ((), ())), preferred_element_type=F32)


def exchange_kernel(
    inputs, ocot, vcot, first, second, lambdas, gain, vf, of, vw, ow, vm, vs, om, os_,
    wv_f, wo_f, da, db, low_v,
    in_v, oc_v, vc_v, fi_v, se_v, vf_v, of_v, vw_v, ow_v, mom_v, sec_v,
    pair, ax, sx, rx, pq, heads,
    la, lb, ra, rb, sa, sb, ra2, rb2, wv, wo,
    load_sem,
    pair_s, pair_r, xs_s, xs_r, xg_s, xg_r, fw_s, fw_r,
    r1a_s, r1a_r, r1b_s, r1b_r, r2a_s, r2a_r, r2b_s, r2b_r,
    g1a_s, g1a_r, g1b_s, g1b_r, g2a_s, g2a_r, g2b_s, g2b_r,
    w1v_s, w1v_r, w1o_s, w1o_r, wrv_s, wrv_r, wro_s, wro_r,
):
    fs = lax.axis_index("fs")
    tp = lax.axis_index("tp")
    z, y = fs // Y, lax.rem(fs, Y)
    x, c = tp // C, lax.rem(tp, C)

    def at_x(d):
        return (fs, lax.rem(x + d, X) * C + c)

    def at_y(d):
        return (z * Y + lax.rem(y + d, Y), tp)

    def at_z(d):
        return (lax.rem(z + d, Z) * Y + y, tp)

    partner = (fs, x * C + (1 - c))

    def send(src, dst, s, r, where):
        copy = pltpu.make_async_remote_copy(
            src_ref=src, dst_ref=dst, send_sem=s, recv_sem=r, device_id=where, device_id_type=MESH
        )
        copy.start()
        return copy

    barrier = pltpu.get_barrier_semaphore()
    friends = (
        [at_y(d) for d in FAR] + [at_z(d) for d in FAR] + [at_x(d) for d in (2, 1, 3)] + [partner]
    )
    for friend in friends:
        pl.semaphore_signal(barrier, inc=1, device_id=friend, device_id_type=MESH)

    chip_rows = pl.ds(pl.multiple_of(x * (C * 256), C * 256), C * 256)
    loads = {}
    for i, (name, src, dst) in enumerate(
        [
            ("vw", vw, vw_v),
            ("ow", ow, ow_v),
            ("in", inputs, in_v),
            ("vf", vf.at[chip_rows], vf_v),
            ("oc", ocot, oc_v),
            ("of", of.at[chip_rows], of_v),
            ("fi", first, fi_v),
            ("se", second, se_v),
            ("vc", vcot, vc_v),
            ("vm", vm, mom_v.at[pl.ds(0, 4)]),
            ("om", om, mom_v.at[pl.ds(4, 4)]),
            ("vs", vs, sec_v.at[pl.ds(0, 4)]),
            ("os", os_, sec_v.at[pl.ds(4, 4)]),
        ]
    ):
        loads[name] = pltpu.make_async_copy(src, dst, load_sem.at[i])
        loads[name].start()

    mine = pl.ds(pl.multiple_of(c * 256, 256), 256)
    theirs = pl.ds(pl.multiple_of((1 - c) * 256, 256), 256)
    pl.semaphore_wait(barrier, len(friends))
    to_pair = [
        send(inputs.at[theirs], pair.at[0], pair_s.at[0], pair_r.at[0], partner),
        send(ocot.at[theirs], pair.at[1], pair_s.at[1], pair_r.at[1], partner),
    ]
    loads["vw"].wait()
    wv[z, y] = encode(vw_v[...], WEIGHT_RATE)
    loads["ow"].wait()
    wo[z, y] = encode(ow_v[...], WEIGHT_RATE)
    w1v, w1o = {}, {}
    for d in FAR:
        w1v[d] = send(wv.at[z, y], wv.at[z, y], w1v_s.at[d], w1v_r.at[d], at_y(d))
        w1o[d] = send(wo.at[z, y], wo.at[z, y], w1o_s.at[d], w1o_r.at[d], at_z(d))
    for name in ("in", "vf", "oc", "of"):
        loads[name].wait()
    acc_p = jnp.dot(in_v[mine], vf_v[mine], preferred_element_type=F32)
    acc_q = jnp.dot(oc_v[mine], of_v[mine], preferred_element_type=F32)
    for copy in to_pair:
        copy.wait_recv()
    acc_p += jnp.dot(pair[0], vf_v[theirs], preferred_element_type=F32)
    acc_q += jnp.dot(pair[1], of_v[theirs], preferred_element_type=F32)
    acc = jnp.concatenate([acc_p, acc_q], axis=1).reshape(X, 64, 512)
    ax[...] = acc
    sx[...] = acc.astype(BF16)
    x_sum = {
        d: send(sx.at[lax.rem(x + d, X)], rx.at[x], xs_s.at[d], xs_r.at[d], at_x(d))
        for d in (2, 1, 3)
    }

    def ring_step(s, h):
        half = pl.ds(h * 4, 4)
        moves = []
        if s < 4 or h == 0:
            zz, yy = lax.rem(z + Z - (s - 1), Z), lax.rem(y + Y - (s - 1), Y)
            k = 4 * (s - 1) + 2 * h
            moves += [(wv.at[zz, half], wrv_s, wrv_r, k, at_z(1))]
            moves += [(wo.at[half, pl.ds(yy, 1)], wro_s, wro_r, k, at_y(1))]
        if s < 4 or h == 1:
            zz, yy = lax.rem(z + (s - 1), Z), lax.rem(y + (s - 1), Y)
            k = 4 * (s - 1) + 2 * h + 1
            moves += [(wv.at[zz, half], wrv_s, wrv_r, k, at_z(Z - 1))]
            moves += [(wo.at[half, pl.ds(yy, 1)], wro_s, wro_r, k, at_y(Y - 1))]
        rings[s, h] = [
            send(ref, ref, ss.at[k], rs.at[k], where) for ref, ss, rs, k, where in moves
        ]

    def ring_wait(s, h):
        for copy in rings[s, h]:
            copy.wait_recv()

    rings = {}

    def open_group(at):
        wv_f[at] = decode(wv[at].reshape(256, 256), WEIGHT_RATE)

    for d in NEAR:
        w1v[d].wait_recv()
        w1o[d].wait_recv()
    ring_step(1, 0)
    ring_step(1, 1)

    loads["fi"].wait()
    loads["se"].wait()
    for h in range(2):
        cols = slice(h * HEAD, (h + 1) * HEAD)
        difference = fi_v[:, cols].astype(F32) - lambdas[h] * se_v[:, cols].astype(F32)
        mean = jnp.mean(difference * difference, axis=-1, keepdims=True)
        heads[:, cols] = (difference * lax.rsqrt(mean + 1e-06) * gain[...]).astype(BF16)

    total = ax[x]
    for d in (1, 3, 2):
        x_sum[d].wait_recv()
        total += rx[lax.rem(x + X - d, X)].astype(F32)
    pq[c, x] = total.astype(BF16)
    x_all = {
        d: send(pq.at[c, x], pq.at[c, x], xg_s.at[d], xg_r.at[d], at_x(d)) for d in (2, 1, 3)
    }
    passed = [send(pq.at[c, x], pq.at[c, x], fw_s.at[0], fw_r.at[0], partner)]

    for s in (1, 2):
        for h in (0, 1):
            ring_wait(s, h)
            ring_step(s + 1, h)

    for d in (1, 3, 2):
        x_all[d].wait_recv()
        xx = lax.rem(x + X - d, X)
        passed.append(send(pq.at[c, xx], pq.at[c, xx], fw_s.at[d], fw_r.at[d], partner))
    loads["vc"].wait()
    pq_mine = pq[c].reshape(256, 512)
    lv = rows_dot(pq_mine[:, :RANK], vc_v[mine])
    lo = rows_dot(pq_mine[:, RANK:], heads[mine])
    for copy in passed:
        copy.wait_recv()
    pq_theirs = pq[1 - c].reshape(256, 512)
    lv += rows_dot(pq_theirs[:, :RANK], vc_v[theirs])
    lo += rows_dot(pq_theirs[:, RANK:], heads[theirs])
    scale = 1.0 / math.sqrt(32768.0)
    lv3 = (lv * scale).reshape(32, 8, 256)
    lo3 = (lo * scale).reshape(32, 8, 256)
    upper = lax.broadcasted_iota(jnp.int32, (32, 8, 256), 1) < 4
    even = jnp.where(upper, lv3, pltpu.roll(lo3, 4, 1)).astype(BF16)
    odd = jnp.where(upper, pltpu.roll(lv3, 4, 1), lo3).astype(BF16)
    for f in range(Z * Y):
        block = (odd if f % 2 else even)[f // 2]
        la[f // Y, f % Y] = block[:, :128]
        lb[f % Y, f // Y] = block[:, 128:]
    r1a, r1b = {}, {}
    for d in FAR:
        r1a[d] = send(la.at[lax.rem(z + d, Z)], ra.at[z], r1a_s.at[d], r1a_r.at[d], at_z(d))
        r1b[d] = send(lb.at[lax.rem(y + d, Y)], rb.at[y], r1b_s.at[d], r1b_r.at[d], at_y(d))

    open_group(z)
    open_group(lax.rem(z + Z - 1, Z))
    open_group(lax.rem(z + 1, Z))
    ring_wait(3, 0)
    ring_step(4, 0)
    ring_wait(3, 1)
    ring_step(4, 1)
    open_group(lax.rem(z + Z - 2, Z))
    open_group(lax.rem(z + 2, Z))
    open_group(lax.rem(z + Z - 3, Z))
    open_group(lax.rem(z + 3, Z))
    ring_wait(4, 0)
    ring_wait(4, 1)
    open_group(lax.rem(z + 4, Z))

    sum_a = la[z].astype(F32)
    sum_b = lb[y].astype(F32)
    for d in NEAR:
        r1a[d].wait_recv()
        sum_a += ra[lax.rem(z + Z - d, Z)].astype(F32)
        r1b[d].wait_recv()
        sum_b += rb[lax.rem(y + Y - d, Y)].astype(F32)
    sa[...] = sum_a
    sb[...] = sum_b
    r2a, r2b = {}, {}
    for d in FAR:
        r2a[d] = send(sa.at[lax.rem(y + d, Y)], ra2.at[y], r2a_s.at[d], r2a_r.at[d], at_y(d))
        r2b[d] = send(sb.at[lax.rem(z + d, Z)], rb2.at[z], r2b_s.at[d], r2b_r.at[d], at_z(d))

    for k in range(Z // 2):
        wo_f[:, k * 256 : (k + 1) * 256] = decode(wo[k].reshape(256, 256).T, WEIGHT_RATE)

    low_a = sa[y]
    low_b = sb[z]
    for d in NEAR:
        r2a[d].wait_recv()
        low_a += ra2[lax.rem(y + Y - d, Y)]
        r2b[d].wait_recv()
        low_b += rb2[lax.rem(z + Z - d, Z)]
    low = jnp.concatenate([low_a, low_b], axis=1)
    low_v[...] = low
    for name in ("vm", "om", "vs", "os"):
        loads[name].wait()
    moment = 0.8 * mom_v[...] + 0.2 * low
    spread = 0.95 * sec_v[...] + 0.05 * low * low
    code = encode(moment / (jnp.sqrt(spread) + 1e-08), DIRECTION_RATE)
    da[z, y] = code[:, :128]
    db[y, z] = code[:, 128:]
    g1a, g1b, g2a, g2b = {}, {}, {}, {}
    for d in FAR:
        g1a[d] = send(da.at[z, y], da.at[z, y], g1a_s.at[d], g1a_r.at[d], at_y(d))
        g1b[d] = send(db.at[y, z], db.at[y, z], g1b_s.at[d], g1b_r.at[d], at_z(d))

    for k in range(Z // 2, Z):
        wo_f[:, k * 256 : (k + 1) * 256] = decode(wo[k].reshape(256, 256).T, WEIGHT_RATE)
    for d in NEAR:
        g1a[d].wait_recv()
    for d in FAR:
        g2a[d] = send(da.at[z], da.at[z], g2a_s.at[d], g2a_r.at[d], at_z(d))
    for d in NEAR:
        g1b[d].wait_recv()
    for d in FAR:
        g2b[d] = send(db.at[y], db.at[y], g2b_s.at[d], g2b_r.at[d], at_y(d))
    for d in NEAR:
        g2a[d].wait_recv()
        g2b[d].wait_recv()
    sent = to_pair + passed
    for group in (w1v, w1o, x_sum, x_all, r1a, r1b, r2a, r2b, g1a, g1b, g2a, g2b):
        sent += list(group.values())
    for ring in rings.values():
        sent += ring
    for copy in sent:
        copy.wait_send()


def finish_kernel(
    da, db, wv, wo, low, vf, of, vw, ow, vm, vs, om, os_,
    vmaster, omaster, vm_new, vs_new, om_new, os_new, vcopy, ocopy,
    dv, do, do_t, vc_v, oc_v, n_v, k_v, out_sem, chunk_sem,
):
    fs = lax.axis_index("fs")
    upper = lax.broadcasted_iota(jnp.int32, (8, 256), 0) < 4
    for g in range(Z * Y // 2):
        zz, yy = (2 * g) // Y, (2 * g) % Y
        even = jnp.concatenate([da[zz, yy], db[yy, zz]], axis=1)
        odd = jnp.concatenate([da[zz, yy + 1], db[yy + 1, zz]], axis=1)
        even = 0.05 * decode(even, DIRECTION_RATE)
        odd = 0.05 * decode(odd, DIRECTION_RATE)
        value = jnp.where(upper, even, pltpu.roll(odd, 4, 0))
        output = jnp.where(upper, pltpu.roll(even, 4, 0), odd)
        for full, both in ((value, dv), (output, do)):
            top = full.astype(BF16)
            both[8 * g : 8 * g + 8] = top
            both[RANK + 8 * g : RANK + 8 * g + 8] = (full - top.astype(F32)).astype(BF16)
    do_t[...] = do[...].T
    outs = []

    def put(src, dst, sem):
        copy = pltpu.make_async_copy(src, dst, sem)
        copy.start()
        outs.append(copy)

    for k in range(CHUNKS):
        rows = pl.ds(k * STEP, STEP)
        factor = vf[rows]
        step = jnp.dot(
            jnp.concatenate([factor, factor], axis=1), dv[...], preferred_element_type=F32
        )
        vc_v[rows] = (wv[rows] - step).astype(BF16)
        put(vc_v.at[rows], vcopy.at[rows], chunk_sem.at[k])
    for k in range(CHUNKS):
        rows = pl.ds(k * STEP, STEP)
        factor = of[rows]
        step = lax.dot_general(
            do_t[...],
            jnp.concatenate([factor, factor], axis=1),
            (((1,), (1,)), ((), ())),
            preferred_element_type=F32,
        )
        oc_v[:, rows] = (wo[:, rows] - step).astype(BF16)
        put(oc_v.at[:, rows], ocopy.at[:, rows], chunk_sem.at[CHUNKS + k])
        if k == 0:
            low_v, low_o = low[0:4], low[4:8]
            n_v[0] = 0.8 * vm[...] + 0.2 * low_v
            n_v[1] = 0.95 * vs[...] + 0.05 * low_v * low_v
            n_v[2] = 0.8 * om[...] + 0.2 * low_o
            n_v[3] = 0.95 * os_[...] + 0.05 * low_o * low_o
            for i, dst in enumerate((vm_new, vs_new, om_new, os_new)):
                put(n_v.at[i], dst, out_sem.at[i])
    own = pl.ds(pl.multiple_of(fs * WIDTH_ROWS, WIDTH_ROWS), WIDTH_ROWS)
    for i, (factor, both, weight, out) in enumerate(
        ((vf, dv, vw, vmaster), (of, do, ow, omaster))
    ):
        rows = factor[own]
        k_v[i] = weight[...] - jnp.dot(
            jnp.concatenate([rows, rows], axis=1), both[...], preferred_element_type=F32
        )
        put(k_v.at[i], out, out_sem.at[4 + i])
    for copy in outs:
        copy.wait()


def local(
    inputs, value_cotangent, first_map, second_map, lambdas, head_gain, output_cotangent,
    value_factor, output_factor, value_weight, output_weight,
    value_moment, value_second, output_moment, output_second,
):
    turned_weight = output_weight.T
    gain = head_gain.reshape(1, HEAD)
    hbm = pl.BlockSpec(memory_space=pltpu.HBM)
    near = pl.BlockSpec(memory_space=pltpu.VMEM)
    dma = pltpu.SemaphoreType.DMA
    vmem = pltpu.VMEM
    sems = [dma((13,)), dma((2,)), dma((2,)), dma((4,)), dma((4,)), dma((4,)), dma((4,)), dma((4,)), dma((4,))]
    sems += [dma((8,))] * 20 + [dma((16,))] * 4
    far = [
        pltpu.with_memory_space_constraint(a, pltpu.HBM)
        for a in (
            inputs, output_cotangent, value_cotangent, first_map, second_map, lambdas, gain,
            value_factor, output_factor, value_weight, turned_weight,
            value_moment, value_second, output_moment, output_second,
        )
    ]
    wv, wo, da, db, low = pl.pallas_call(
        exchange_kernel,
        out_shape=[
            jax.ShapeDtypeStruct((Z, 256, 256), F32),
            jax.ShapeDtypeStruct((256, 2048), F32),
            jax.ShapeDtypeStruct((Z, Y, 8, 128), BF16),
            jax.ShapeDtypeStruct((Y, Z, 8, 128), BF16),
            jax.ShapeDtypeStruct((8, 256), F32),
        ],
        in_specs=[hbm] * 5
        + [pl.BlockSpec(memory_space=pltpu.SMEM), pl.BlockSpec(memory_space=pltpu.VMEM)]
        + [hbm] * 8,
        out_specs=[near] * 5,
        scratch_shapes=[
            vmem((512, 256), BF16), vmem((512, 256), BF16), vmem((512, 256), BF16),
            vmem((512, 256), BF16), vmem((512, 256), BF16),
            vmem((512, 256), BF16), vmem((512, 256), BF16),
            vmem((WIDTH_ROWS, 256), F32), vmem((WIDTH_ROWS, 256), F32),
            vmem((8, 256), F32), vmem((8, 256), F32),
            vmem((2, 256, 256), BF16), vmem((X, 64, 512), F32), vmem((X, 64, 512), BF16),
            vmem((X, 64, 512), BF16), vmem((C, X, 64, 512), BF16), vmem((512, 256), BF16),
            vmem((Z, Y, 8, 128), BF16), vmem((Y, Z, 8, 128), BF16),
            vmem((Z, Y, 8, 128), BF16), vmem((Y, Z, 8, 128), BF16),
            vmem((Y, 8, 128), F32), vmem((Z, 8, 128), F32),
            vmem((Y, 8, 128), F32), vmem((Z, 8, 128), F32),
            vmem((Z, Y, WIDTH_ROWS, 256), BF16), vmem((Z, Y, WIDTH_ROWS, 256), BF16),
        ]
        + sems,
        compiler_params=pltpu.CompilerParams(
            collective_id=0, has_side_effects=True, vmem_limit_bytes=24 * 1024 * 1024
        ),
        name="exchange",
    )(*far)
    width, cols = 2048, 256
    wv = wv.reshape(width, cols)

    small = jax.ShapeDtypeStruct((4, cols), F32)
    own = jax.ShapeDtypeStruct((WIDTH_ROWS, cols), F32)
    vmaster, omaster, *rest = pl.pallas_call(
        finish_kernel,
        out_shape=[
            own, own, small, small, small, small,
            jax.ShapeDtypeStruct((width, cols), BF16),
            jax.ShapeDtypeStruct((cols, width), BF16),
        ],
        in_specs=[near] * 13,
        out_specs=[hbm] * 8,
        scratch_shapes=[
            vmem((2 * RANK, cols), BF16), vmem((2 * RANK, cols), BF16), vmem((cols, 2 * RANK), BF16),
            vmem((width, cols), BF16), vmem((cols, width), BF16),
            vmem((4, 4, cols), F32), vmem((2, WIDTH_ROWS, cols), F32),
            dma((6,)), dma((2 * CHUNKS,)),
        ],
        compiler_params=pltpu.CompilerParams(vmem_limit_bytes=24 * 1024 * 1024),
        name="finish",
    )(
        da, db, wv, wo, low, value_factor, output_factor, value_weight, turned_weight,
        value_moment, value_second, output_moment, output_second,
    )
    return (vmaster, omaster.T, *rest)


def solution(mesh):
    both = P("fs", "tp")
    in_specs = (
        both, both, both, both, P("tp"), P(), both, P(), P(), both, P("tp", "fs"),
        both, both, both, both,
    )
    out_specs = (
        both, P("tp", "fs"), both, both, both, both, P(None, "tp"), P("tp", None),
    )
    return jax.shard_map(local, mesh=mesh, in_specs=in_specs, out_specs=out_specs, check_vma=False)
```

```python
import functools
import math

import jax
import jax.numpy as jnp
from jax import lax
from jax.experimental import pallas as pl
from jax.experimental.pallas import tpu as pltpu
from jax.sharding import PartitionSpec as P

MESH = pl.DeviceIdType.MESH
X, C, Y, Z = 4, 2, 8, 8
F32, BF16 = jnp.float32, jnp.bfloat16
RANK, HEAD = 256, 128
FAR = (4, 3, 5, 2, 6, 1, 7)
NEAR = (1, 7, 2, 6, 3, 5, 4)
WIDTH_ROWS = 32
STEP = 512
CHUNKS = 2048 // STEP
WEIGHT_RATE = 960.0
DIRECTION_RATE = 11.0


def encode(value, rate):
    size = jnp.exp2(jnp.abs(value) * rate) - 1.0
    return jnp.where(value < 0, -size, size).astype(BF16)


def decode(code, rate):
    code = code.astype(F32)
    size = jnp.log(1.0 + jnp.abs(code)) * (1.0 / (rate * math.log(2.0)))
    return jnp.where(code < 0, -size, size)


def rows_dot(left, right):
    return lax.dot_general(left, right, (((0,), (0,)), ((), ())), preferred_element_type=F32)


def exchange_kernel(
    inputs, ocot, vcot, first, second, lambdas, gain, vf, of, vw, ow, vm, vs, om, os_,
    wv_f, wo_f, da, db, low_v,
    in_v, oc_v, vc_v, fi_v, se_v, vf_v, of_v, vw_v, ow_v, mom_v, sec_v,
    pair, ax, sx, rx, pq, heads,
    la, lb, ra, rb, sa, sb, ra2, rb2, wv, wo,
    load_sem,
    pair_s, pair_r, xs_s, xs_r, xg_s, xg_r, fw_s, fw_r,
    r1a_s, r1a_r, r1b_s, r1b_r, r2a_s, r2a_r, r2b_s, r2b_r,
    g1a_s, g1a_r, g1b_s, g1b_r, g2a_s, g2a_r, g2b_s, g2b_r,
    w1v_s, w1v_r, w1o_s, w1o_r, wrv_s, wrv_r, wro_s, wro_r,
):
    fs = lax.axis_index("fs")
    tp = lax.axis_index("tp")
    z, y = fs // Y, lax.rem(fs, Y)
    x, c = tp // C, lax.rem(tp, C)

    def at_x(d):
        return (fs, lax.rem(x + d, X) * C + c)

    def at_y(d):
        return (z * Y + lax.rem(y + d, Y), tp)

    def at_z(d):
        return (lax.rem(z + d, Z) * Y + y, tp)

    partner = (fs, x * C + (1 - c))

    def send(src, dst, s, r, where):
        copy = pltpu.make_async_remote_copy(
            src_ref=src, dst_ref=dst, send_sem=s, recv_sem=r, device_id=where, device_id_type=MESH
        )
        copy.start()
        return copy

    barrier = pltpu.get_barrier_semaphore()
    friends = (
        [at_y(d) for d in FAR] + [at_z(d) for d in FAR] + [at_x(d) for d in (2, 1, 3)] + [partner]
    )
    for friend in friends:
        pl.semaphore_signal(barrier, inc=1, device_id=friend, device_id_type=MESH)

    chip_rows = pl.ds(pl.multiple_of(x * (C * 256), C * 256), C * 256)
    loads = {}
    for i, (name, src, dst) in enumerate(
        [
            ("vw", vw, vw_v),
            ("ow", ow, ow_v),
            ("in", inputs, in_v),
            ("vf", vf.at[chip_rows], vf_v),
            ("oc", ocot, oc_v),
            ("of", of.at[chip_rows], of_v),
            ("fi", first, fi_v),
            ("se", second, se_v),
            ("vc", vcot, vc_v),
            ("vm", vm, mom_v.at[pl.ds(0, 4)]),
            ("om", om, mom_v.at[pl.ds(4, 4)]),
            ("vs", vs, sec_v.at[pl.ds(0, 4)]),
            ("os", os_, sec_v.at[pl.ds(4, 4)]),
        ]
    ):
        loads[name] = pltpu.make_async_copy(src, dst, load_sem.at[i])
        loads[name].start()

    mine = pl.ds(pl.multiple_of(c * 256, 256), 256)
    theirs = pl.ds(pl.multiple_of((1 - c) * 256, 256), 256)
    pl.semaphore_wait(barrier, len(friends))
    to_pair = [
        send(inputs.at[theirs], pair.at[0], pair_s.at[0], pair_r.at[0], partner),
        send(ocot.at[theirs], pair.at[1], pair_s.at[1], pair_r.at[1], partner),
    ]
    loads["vw"].wait()
    wv[z, y] = encode(vw_v[...], WEIGHT_RATE)
    loads["ow"].wait()
    wo[z, y] = encode(ow_v[...], WEIGHT_RATE)
    w1v, w1o = {}, {}
    for d in FAR:
        w1v[d] = send(wv.at[z, y], wv.at[z, y], w1v_s.at[d], w1v_r.at[d], at_y(d))
        w1o[d] = send(wo.at[z, y], wo.at[z, y], w1o_s.at[d], w1o_r.at[d], at_z(d))
    for name in ("in", "vf", "oc", "of"):
        loads[name].wait()
    acc_p = jnp.dot(in_v[mine], vf_v[mine], preferred_element_type=F32)
    acc_q = jnp.dot(oc_v[mine], of_v[mine], preferred_element_type=F32)
    for copy in to_pair:
        copy.wait_recv()
    acc_p += jnp.dot(pair[0], vf_v[theirs], preferred_element_type=F32)
    acc_q += jnp.dot(pair[1], of_v[theirs], preferred_element_type=F32)
    acc = jnp.concatenate([acc_p, acc_q], axis=1).reshape(X, 64, 512)
    ax[...] = acc
    sx[...] = acc.astype(BF16)
    x_sum = {
        d: send(sx.at[lax.rem(x + d, X)], rx.at[x], xs_s.at[d], xs_r.at[d], at_x(d))
        for d in (2, 1, 3)
    }

    def ring_step(s, h):
        half = pl.ds(h * 4, 4)
        moves = []
        if s < 4 or h == 0:
            zz, yy = lax.rem(z + Z - (s - 1), Z), lax.rem(y + Y - (s - 1), Y)
            k = 4 * (s - 1) + 2 * h
            moves += [(wv.at[zz, half], wrv_s, wrv_r, k, at_z(1))]
            moves += [(wo.at[half, pl.ds(yy, 1)], wro_s, wro_r, k, at_y(1))]
        if s < 4 or h == 1:
            zz, yy = lax.rem(z + (s - 1), Z), lax.rem(y + (s - 1), Y)
            k = 4 * (s - 1) + 2 * h + 1
            moves += [(wv.at[zz, half], wrv_s, wrv_r, k, at_z(Z - 1))]
            moves += [(wo.at[half, pl.ds(yy, 1)], wro_s, wro_r, k, at_y(Y - 1))]
        rings[s, h] = [
            send(ref, ref, ss.at[k], rs.at[k], where) for ref, ss, rs, k, where in moves
        ]

    def ring_wait(s, h):
        for copy in rings[s, h]:
            copy.wait_recv()

    rings = {}

    def open_group(at):
        wv_f[at] = decode(wv[at].reshape(256, 256), WEIGHT_RATE)

    for d in NEAR:
        w1v[d].wait_recv()
        w1o[d].wait_recv()
    ring_step(1, 0)
    ring_step(1, 1)

    loads["fi"].wait()
    loads["se"].wait()
    for h in range(2):
        cols = slice(h * HEAD, (h + 1) * HEAD)
        difference = fi_v[:, cols].astype(F32) - lambdas[h] * se_v[:, cols].astype(F32)
        mean = jnp.mean(difference * difference, axis=-1, keepdims=True)
        heads[:, cols] = (difference * lax.rsqrt(mean + 1e-06) * gain[...]).astype(BF16)

    total = ax[x]
    for d in (1, 3, 2):
        x_sum[d].wait_recv()
        total += rx[lax.rem(x + X - d, X)].astype(F32)
    pq[c, x] = total.astype(BF16)
    x_all = {
        d: send(pq.at[c, x], pq.at[c, x], xg_s.at[d], xg_r.at[d], at_x(d)) for d in (2, 1, 3)
    }
    passed = [send(pq.at[c, x], pq.at[c, x], fw_s.at[0], fw_r.at[0], partner)]

    ring_wait(1, 0)
    ring_step(2, 0)
    ring_wait(1, 1)
    ring_step(2, 1)

    for d in (1, 3, 2):
        x_all[d].wait_recv()
        xx = lax.rem(x + X - d, X)
        passed.append(send(pq.at[c, xx], pq.at[c, xx], fw_s.at[d], fw_r.at[d], partner))
    loads["vc"].wait()
    pq_mine = pq[c].reshape(256, 512)
    lv = rows_dot(pq_mine[:, :RANK], vc_v[mine])
    lo = rows_dot(pq_mine[:, RANK:], heads[mine])
    for copy in passed:
        copy.wait_recv()
    pq_theirs = pq[1 - c].reshape(256, 512)
    lv += rows_dot(pq_theirs[:, :RANK], vc_v[theirs])
    lo += rows_dot(pq_theirs[:, RANK:], heads[theirs])
    scale = 1.0 / math.sqrt(32768.0)
    lv3 = (lv * scale).reshape(32, 8, 256)
    lo3 = (lo * scale).reshape(32, 8, 256)
    upper = lax.broadcasted_iota(jnp.int32, (32, 8, 256), 1) < 4
    even = jnp.where(upper, lv3, pltpu.roll(lo3, 4, 1)).astype(BF16)
    odd = jnp.where(upper, pltpu.roll(lv3, 4, 1), lo3).astype(BF16)
    for f in range(Z * Y):
        block = (odd if f % 2 else even)[f // 2]
        la[f // Y, f % Y] = block[:, :128]
        lb[f % Y, f // Y] = block[:, 128:]
    r1a, r1b = {}, {}
    for d in FAR:
        r1a[d] = send(la.at[lax.rem(z + d, Z)], ra.at[z], r1a_s.at[d], r1a_r.at[d], at_z(d))
        r1b[d] = send(lb.at[lax.rem(y + d, Y)], rb.at[y], r1b_s.at[d], r1b_r.at[d], at_y(d))

    ring_wait(2, 0)
    ring_step(3, 0)
    ring_wait(2, 1)
    ring_step(3, 1)
    open_group(z)
    open_group(lax.rem(z + Z - 1, Z))
    open_group(lax.rem(z + 1, Z))
    sum_a = la[z].astype(F32)
    sum_b = lb[y].astype(F32)
    for d in NEAR:
        r1a[d].wait_recv()
        sum_a += ra[lax.rem(z + Z - d, Z)].astype(F32)
        r1b[d].wait_recv()
        sum_b += rb[lax.rem(y + Y - d, Y)].astype(F32)
    sa[...] = sum_a
    sb[...] = sum_b
    r2a, r2b = {}, {}
    for d in FAR:
        r2a[d] = send(sa.at[lax.rem(y + d, Y)], ra2.at[y], r2a_s.at[d], r2a_r.at[d], at_y(d))
        r2b[d] = send(sb.at[lax.rem(z + d, Z)], rb2.at[z], r2b_s.at[d], r2b_r.at[d], at_z(d))

    ring_wait(3, 0)
    ring_step(4, 0)
    ring_wait(3, 1)
    ring_step(4, 1)
    open_group(lax.rem(z + Z - 2, Z))
    open_group(lax.rem(z + 2, Z))

    low_a = sa[y]
    low_b = sb[z]
    for d in NEAR:
        r2a[d].wait_recv()
        low_a += ra2[lax.rem(y + Y - d, Y)]
        r2b[d].wait_recv()
        low_b += rb2[lax.rem(z + Z - d, Z)]
    low = jnp.concatenate([low_a, low_b], axis=1)
    low_v[...] = low
    for name in ("vm", "om", "vs", "os"):
        loads[name].wait()
    moment = 0.8 * mom_v[...] + 0.2 * low
    spread = 0.95 * sec_v[...] + 0.05 * low * low
    code = encode(moment / (jnp.sqrt(spread) + 1e-08), DIRECTION_RATE)
    da[z, y] = code[:, :128]
    db[y, z] = code[:, 128:]
    g1a, g1b, g2a, g2b = {}, {}, {}, {}
    for d in FAR:
        g1a[d] = send(da.at[z, y], da.at[z, y], g1a_s.at[d], g1a_r.at[d], at_y(d))
        g1b[d] = send(db.at[y, z], db.at[y, z], g1b_s.at[d], g1b_r.at[d], at_z(d))

    ring_wait(4, 0)
    ring_wait(4, 1)
    open_group(lax.rem(z + 4, Z))
    open_group(lax.rem(z + Z - 3, Z))
    open_group(lax.rem(z + 3, Z))
    for k in range(Z):
        wo_f[:, k * 256 : (k + 1) * 256] = decode(wo[k].reshape(256, 256).T, WEIGHT_RATE)
    for d in NEAR:
        g1a[d].wait_recv()
    for d in FAR:
        g2a[d] = send(da.at[z], da.at[z], g2a_s.at[d], g2a_r.at[d], at_z(d))
    for d in NEAR:
        g1b[d].wait_recv()
    for d in FAR:
        g2b[d] = send(db.at[y], db.at[y], g2b_s.at[d], g2b_r.at[d], at_y(d))
    for d in NEAR:
        g2a[d].wait_recv()
        g2b[d].wait_recv()
    sent = to_pair + passed
    for group in (w1v, w1o, x_sum, x_all, r1a, r1b, r2a, r2b, g1a, g1b, g2a, g2b):
        sent += list(group.values())
    for ring in rings.values():
        sent += ring
    for copy in sent:
        copy.wait_send()


def finish_kernel(
    da, db, wv, wo, low, vf, of, vw, ow, vm, vs, om, os_,
    vmaster, omaster, vm_new, vs_new, om_new, os_new, vcopy, ocopy,
    dv, do, do_t, vc_v, oc_v, n_v, k_v, out_sem, chunk_sem,
):
    fs = lax.axis_index("fs")
    upper = lax.broadcasted_iota(jnp.int32, (8, 256), 0) < 4
    for g in range(Z * Y // 2):
        zz, yy = (2 * g) // Y, (2 * g) % Y
        even = jnp.concatenate([da[zz, yy], db[yy, zz]], axis=1)
        odd = jnp.concatenate([da[zz, yy + 1], db[yy + 1, zz]], axis=1)
        even = 0.05 * decode(even, DIRECTION_RATE)
        odd = 0.05 * decode(odd, DIRECTION_RATE)
        value = jnp.where(upper, even, pltpu.roll(odd, 4, 0))
        output = jnp.where(upper, pltpu.roll(even, 4, 0), odd)
        for full, both in ((value, dv), (output, do)):
            top = full.astype(BF16)
            both[8 * g : 8 * g + 8] = top
            both[RANK + 8 * g : RANK + 8 * g + 8] = (full - top.astype(F32)).astype(BF16)
    do_t[...] = do[...].T
    outs = []

    def put(src, dst, sem):
        copy = pltpu.make_async_copy(src, dst, sem)
        copy.start()
        outs.append(copy)

    for k in range(CHUNKS):
        rows = pl.ds(k * STEP, STEP)
        factor = vf[rows]
        step = jnp.dot(
            jnp.concatenate([factor, factor], axis=1), dv[...], preferred_element_type=F32
        )
        vc_v[rows] = (wv[rows] - step).astype(BF16)
        put(vc_v.at[rows], vcopy.at[rows], chunk_sem.at[k])
    for k in range(CHUNKS):
        rows = pl.ds(k * STEP, STEP)
        factor = of[rows]
        step = lax.dot_general(
            do_t[...],
            jnp.concatenate([factor, factor], axis=1),
            (((1,), (1,)), ((), ())),
            preferred_element_type=F32,
        )
        oc_v[:, rows] = (wo[:, rows] - step).astype(BF16)
        put(oc_v.at[:, rows], ocopy.at[:, rows], chunk_sem.at[CHUNKS + k])
        if k == 0:
            low_v, low_o = low[0:4], low[4:8]
            n_v[0] = 0.8 * vm[...] + 0.2 * low_v
            n_v[1] = 0.95 * vs[...] + 0.05 * low_v * low_v
            n_v[2] = 0.8 * om[...] + 0.2 * low_o
            n_v[3] = 0.95 * os_[...] + 0.05 * low_o * low_o
            for i, dst in enumerate((vm_new, vs_new, om_new, os_new)):
                put(n_v.at[i], dst, out_sem.at[i])
    own = pl.ds(pl.multiple_of(fs * WIDTH_ROWS, WIDTH_ROWS), WIDTH_ROWS)
    for i, (factor, both, weight, out) in enumerate(
        ((vf, dv, vw, vmaster), (of, do, ow, omaster))
    ):
        rows = factor[own]
        k_v[i] = weight[...] - jnp.dot(
            jnp.concatenate([rows, rows], axis=1), both[...], preferred_element_type=F32
        )
        put(k_v.at[i], out, out_sem.at[4 + i])
    for copy in outs:
        copy.wait()


def local(
    inputs, value_cotangent, first_map, second_map, lambdas, head_gain, output_cotangent,
    value_factor, output_factor, value_weight, output_weight,
    value_moment, value_second, output_moment, output_second,
):
    turned_weight = output_weight.T
    gain = head_gain.reshape(1, HEAD)
    hbm = pl.BlockSpec(memory_space=pltpu.HBM)
    near = pl.BlockSpec(memory_space=pltpu.VMEM)
    dma = pltpu.SemaphoreType.DMA
    vmem = pltpu.VMEM
    sems = [dma((13,)), dma((2,)), dma((2,)), dma((4,)), dma((4,)), dma((4,)), dma((4,)), dma((4,)), dma((4,))]
    sems += [dma((8,))] * 20 + [dma((16,))] * 4
    far = [
        pltpu.with_memory_space_constraint(a, pltpu.HBM)
        for a in (
            inputs, output_cotangent, value_cotangent, first_map, second_map, lambdas, gain,
            value_factor, output_factor, value_weight, turned_weight,
            value_moment, value_second, output_moment, output_second,
        )
    ]
    wv, wo, da, db, low = pl.pallas_call(
        exchange_kernel,
        out_shape=[
            jax.ShapeDtypeStruct((Z, 256, 256), F32),
            jax.ShapeDtypeStruct((256, 2048), F32),
            jax.ShapeDtypeStruct((Z, Y, 8, 128), BF16),
            jax.ShapeDtypeStruct((Y, Z, 8, 128), BF16),
            jax.ShapeDtypeStruct((8, 256), F32),
        ],
        in_specs=[hbm] * 5
        + [pl.BlockSpec(memory_space=pltpu.SMEM), pl.BlockSpec(memory_space=pltpu.VMEM)]
        + [hbm] * 8,
        out_specs=[near] * 5,
        scratch_shapes=[
            vmem((512, 256), BF16), vmem((512, 256), BF16), vmem((512, 256), BF16),
            vmem((512, 256), BF16), vmem((512, 256), BF16),
            vmem((512, 256), BF16), vmem((512, 256), BF16),
            vmem((WIDTH_ROWS, 256), F32), vmem((WIDTH_ROWS, 256), F32),
            vmem((8, 256), F32), vmem((8, 256), F32),
            vmem((2, 256, 256), BF16), vmem((X, 64, 512), F32), vmem((X, 64, 512), BF16),
            vmem((X, 64, 512), BF16), vmem((C, X, 64, 512), BF16), vmem((512, 256), BF16),
            vmem((Z, Y, 8, 128), BF16), vmem((Y, Z, 8, 128), BF16),
            vmem((Z, Y, 8, 128), BF16), vmem((Y, Z, 8, 128), BF16),
            vmem((Y, 8, 128), F32), vmem((Z, 8, 128), F32),
            vmem((Y, 8, 128), F32), vmem((Z, 8, 128), F32),
            vmem((Z, Y, WIDTH_ROWS, 256), BF16), vmem((Z, Y, WIDTH_ROWS, 256), BF16),
        ]
        + sems,
        compiler_params=pltpu.CompilerParams(
            collective_id=0, has_side_effects=True, vmem_limit_bytes=24 * 1024 * 1024
        ),
        name="exchange",
    )(*far)
    width, cols = 2048, 256
    wv = wv.reshape(width, cols)

    small = jax.ShapeDtypeStruct((4, cols), F32)
    own = jax.ShapeDtypeStruct((WIDTH_ROWS, cols), F32)
    vmaster, omaster, *rest = pl.pallas_call(
        finish_kernel,
        out_shape=[
            own, own, small, small, small, small,
            jax.ShapeDtypeStruct((width, cols), BF16),
            jax.ShapeDtypeStruct((cols, width), BF16),
        ],
        in_specs=[near] * 13,
        out_specs=[hbm] * 8,
        scratch_shapes=[
            vmem((2 * RANK, cols), BF16), vmem((2 * RANK, cols), BF16), vmem((cols, 2 * RANK), BF16),
            vmem((width, cols), BF16), vmem((cols, width), BF16),
            vmem((4, 4, cols), F32), vmem((2, WIDTH_ROWS, cols), F32),
            dma((6,)), dma((2 * CHUNKS,)),
        ],
        compiler_params=pltpu.CompilerParams(vmem_limit_bytes=24 * 1024 * 1024),
        name="finish",
    )(
        da, db, wv, wo, low, value_factor, output_factor, value_weight, turned_weight,
        value_moment, value_second, output_moment, output_second,
    )
    return (vmaster, omaster.T, *rest)


def solution(mesh):
    both = P("fs", "tp")
    in_specs = (
        both, both, both, both, P("tp"), P(), both, P(), P(), both, P("tp", "fs"),
        both, both, both, both,
    )
    out_specs = (
        both, P("tp", "fs"), both, both, both, both, P(None, "tp"), P("tp", None),
    )
    return jax.shard_map(local, mesh=mesh, in_specs=in_specs, out_specs=out_specs, check_vma=False)
```

```python
import functools
import math

import jax
import jax.numpy as jnp
from jax import lax
from jax.experimental import pallas as pl
from jax.experimental.pallas import tpu as pltpu
from jax.sharding import PartitionSpec as P

MESH = pl.DeviceIdType.MESH
X, C, Y, Z = 4, 2, 8, 8
F32, BF16 = jnp.float32, jnp.bfloat16
RANK, HEAD = 256, 128
FAR = (4, 3, 5, 2, 6, 1, 7)
NEAR = (1, 7, 2, 6, 3, 5, 4)
WIDTH_ROWS = 32
STEP = 512
CHUNKS = 2048 // STEP
WEIGHT_RATE = 960.0
DIRECTION_RATE = 11.0


def encode(value, rate):
    size = jnp.exp2(jnp.abs(value) * rate) - 1.0
    return jnp.where(value < 0, -size, size).astype(BF16)


def decode(code, rate):
    code = code.astype(F32)
    size = jnp.log(1.0 + jnp.abs(code)) * (1.0 / (rate * math.log(2.0)))
    return jnp.where(code < 0, -size, size)


def rows_dot(left, right):
    return lax.dot_general(left, right, (((0,), (0,)), ((), ())), preferred_element_type=F32)


def exchange_kernel(
    inputs, ocot, vcot, first, second, lambdas, gain, vf, of, vw, ow, vm, vs, om, os_,
    wv_f, wo_f, da, db, low_v,
    in_v, oc_v, vc_v, fi_v, se_v, vf_v, of_v, vw_v, ow_v, ma, mb,
    pair, ax, sx, rx, pq, heads,
    la, lb, ra, rb, sa, sb, ra2, rb2, wv, wo,
    load_sem,
    pair_s, pair_r, xs_s, xs_r, xg_s, xg_r, fw_s, fw_r,
    r1a_s, r1a_r, r1b_s, r1b_r, r2a_s, r2a_r, r2b_s, r2b_r,
    g1a_s, g1a_r, g1b_s, g1b_r, g2a_s, g2a_r, g2b_s, g2b_r,
    w1v_s, w1v_r, w1o_s, w1o_r, wrv_s, wrv_r, wro_s, wro_r,
):
    fs = lax.axis_index("fs")
    tp = lax.axis_index("tp")
    z, y = fs // Y, lax.rem(fs, Y)
    x, c = tp // C, lax.rem(tp, C)

    def at_x(d):
        return (fs, lax.rem(x + d, X) * C + c)

    def at_y(d):
        return (z * Y + lax.rem(y + d, Y), tp)

    def at_z(d):
        return (lax.rem(z + d, Z) * Y + y, tp)

    partner = (fs, x * C + (1 - c))

    def send(src, dst, s, r, where):
        copy = pltpu.make_async_remote_copy(
            src_ref=src, dst_ref=dst, send_sem=s, recv_sem=r, device_id=where, device_id_type=MESH
        )
        copy.start()
        return copy

    barrier = pltpu.get_barrier_semaphore()
    friends = (
        [at_y(d) for d in FAR] + [at_z(d) for d in FAR] + [at_x(d) for d in (2, 1, 3)] + [partner]
    )
    for friend in friends:
        pl.semaphore_signal(barrier, inc=1, device_id=friend, device_id_type=MESH)

    chip_rows = pl.ds(pl.multiple_of(x * (C * 256), C * 256), C * 256)
    loads = {}
    for i, (name, src, dst) in enumerate(
        [
            ("vw", vw, vw_v),
            ("ow", ow, ow_v),
            ("in", inputs, in_v),
            ("vf", vf.at[chip_rows], vf_v),
            ("oc", ocot, oc_v),
            ("of", of.at[chip_rows], of_v),
            ("fi", first, fi_v),
            ("se", second, se_v),
            ("vc", vcot, vc_v),
        ]
        + [
            (f"{name}{i}", src.at[:, pl.ds(i * 128, 128)], dst.at[kind, pl.ds(row, 4)])
            for i, dst in enumerate((ma.at[y], mb.at[z]))
            for name, src, kind, row in (
                ("vm", vm, 0, 0), ("om", om, 0, 4), ("vs", vs, 1, 0), ("os", os_, 1, 4)
            )
        ]
    ):
        loads[name] = pltpu.make_async_copy(src, dst, load_sem.at[i])
        loads[name].start()

    mine = pl.ds(pl.multiple_of(c * 256, 256), 256)
    theirs = pl.ds(pl.multiple_of((1 - c) * 256, 256), 256)
    pl.semaphore_wait(barrier, len(friends))
    to_pair = [
        send(inputs.at[theirs], pair.at[0], pair_s.at[0], pair_r.at[0], partner),
        send(ocot.at[theirs], pair.at[1], pair_s.at[1], pair_r.at[1], partner),
    ]
    loads["vw"].wait()
    wv[z, y] = encode(vw_v[...], WEIGHT_RATE)
    loads["ow"].wait()
    wo[z, y] = encode(ow_v[...], WEIGHT_RATE)
    w1v, w1o = {}, {}
    for d in FAR:
        w1v[d] = send(wv.at[z, y], wv.at[z, y], w1v_s.at[d], w1v_r.at[d], at_y(d))
        w1o[d] = send(wo.at[z, y], wo.at[z, y], w1o_s.at[d], w1o_r.at[d], at_z(d))
    for name in ("in", "vf", "oc", "of"):
        loads[name].wait()
    for copy in to_pair:
        copy.wait_recv()
    x_sum = {}
    for h in range(2):

        def part(tokens):
            return tokens.reshape(X, 64, 256)[:, h * 32 : (h + 1) * 32].reshape(X * 32, 256)

        acc_p = jnp.dot(part(in_v[mine]), vf_v[mine], preferred_element_type=F32)
        acc_q = jnp.dot(part(oc_v[mine]), of_v[mine], preferred_element_type=F32)
        acc_p += jnp.dot(part(pair[0]), vf_v[theirs], preferred_element_type=F32)
        acc_q += jnp.dot(part(pair[1]), of_v[theirs], preferred_element_type=F32)
        acc = jnp.concatenate([acc_p, acc_q], axis=1).reshape(X, 32, 512)
        ax[h] = acc
        sx[h] = acc.astype(BF16)
        for d in (2, 1, 3):
            k = 4 * h + d
            x_sum[h, d] = send(
                sx.at[h, lax.rem(x + d, X)], rx.at[h, x], xs_s.at[k], xs_r.at[k], at_x(d)
            )

    def ring_step(s, h):
        half = pl.ds(h * 4, 4)
        moves = []
        if s < 4 or h == 0:
            zz, yy = lax.rem(z + Z - (s - 1), Z), lax.rem(y + Y - (s - 1), Y)
            k = 4 * (s - 1) + 2 * h
            moves += [(wv.at[zz, half], wrv_s, wrv_r, k, at_z(1))]
            moves += [(wo.at[half, pl.ds(yy, 1)], wro_s, wro_r, k, at_y(1))]
        if s < 4 or h == 1:
            zz, yy = lax.rem(z + (s - 1), Z), lax.rem(y + (s - 1), Y)
            k = 4 * (s - 1) + 2 * h + 1
            moves += [(wv.at[zz, half], wrv_s, wrv_r, k, at_z(Z - 1))]
            moves += [(wo.at[half, pl.ds(yy, 1)], wro_s, wro_r, k, at_y(Y - 1))]
        rings[s, h] = [
            send(ref, ref, ss.at[k], rs.at[k], where) for ref, ss, rs, k, where in moves
        ]

    def ring_wait(s, h):
        for copy in rings[s, h]:
            copy.wait_recv()

    rings = {}

    def open_group(at):
        wv_f[at] = decode(wv[at].reshape(256, 256), WEIGHT_RATE)

    for d in NEAR:
        w1v[d].wait_recv()
        w1o[d].wait_recv()
    for name in ("vm", "om", "vs", "os"):
        loads[name + "0"].wait()
        loads[name + "1"].wait()
    g1a, g1b = {}, {}
    for d in FAR:
        g1a[d] = send(ma.at[y], ma.at[y], g1a_s.at[d], g1a_r.at[d], at_y(d))
        g1b[d] = send(mb.at[z], mb.at[z], g1b_s.at[d], g1b_r.at[d], at_z(d))
    ring_step(1, 0)
    ring_step(1, 1)

    loads["fi"].wait()
    loads["se"].wait()
    for h in range(2):
        cols = slice(h * HEAD, (h + 1) * HEAD)
        difference = fi_v[:, cols].astype(F32) - lambdas[h] * se_v[:, cols].astype(F32)
        mean = jnp.mean(difference * difference, axis=-1, keepdims=True)
        heads[:, cols] = (difference * lax.rsqrt(mean + 1e-06) * gain[...]).astype(BF16)

    x_all, passed = {}, []
    for h in range(2):
        total = ax[h, x]
        for d in (1, 3, 2):
            x_sum[h, d].wait_recv()
            total += rx[h, lax.rem(x + X - d, X)].astype(F32)
        pq[c, x, h] = total.astype(BF16)
        block = pq.at[c, x, h]
        for d in (2, 1, 3):
            k = 4 * h + d
            x_all[h, d] = send(block, block, xg_s.at[k], xg_r.at[k], at_x(d))
        passed.append(send(block, block, fw_s.at[4 * h], fw_r.at[4 * h], partner))

    ring_wait(1, 0)
    ring_step(2, 0)
    ring_wait(1, 1)
    ring_step(2, 1)

    for h in range(2):
        for d in (1, 3, 2):
            x_all[h, d].wait_recv()
            block = pq.at[c, lax.rem(x + X - d, X), h]
            k = 4 * h + d
            passed.append(send(block, block, fw_s.at[k], fw_r.at[k], partner))
    loads["vc"].wait()
    pq_mine = pq[c].reshape(256, 512)
    lv = rows_dot(pq_mine[:, :RANK], vc_v[mine])
    lo = rows_dot(pq_mine[:, RANK:], heads[mine])
    for copy in passed:
        copy.wait_recv()
    pq_theirs = pq[1 - c].reshape(256, 512)
    lv += rows_dot(pq_theirs[:, :RANK], vc_v[theirs])
    lo += rows_dot(pq_theirs[:, RANK:], heads[theirs])
    scale = 1.0 / math.sqrt(32768.0)
    lv3 = (lv * scale).reshape(32, 8, 256)
    lo3 = (lo * scale).reshape(32, 8, 256)
    upper = lax.broadcasted_iota(jnp.int32, (32, 8, 256), 1) < 4
    even = jnp.where(upper, lv3, pltpu.roll(lo3, 4, 1)).astype(BF16)
    odd = jnp.where(upper, pltpu.roll(lv3, 4, 1), lo3).astype(BF16)
    for f in range(Z * Y):
        block = (odd if f % 2 else even)[f // 2]
        la[f // Y, f % Y] = block[:, :128]
        lb[f % Y, f // Y] = block[:, 128:]
    r1a, r1b = {}, {}
    for d in FAR:
        r1a[d] = send(la.at[lax.rem(z + d, Z)], ra.at[z], r1a_s.at[d], r1a_r.at[d], at_z(d))
        r1b[d] = send(lb.at[lax.rem(y + d, Y)], rb.at[y], r1b_s.at[d], r1b_r.at[d], at_y(d))

    ring_wait(2, 0)
    ring_step(3, 0)
    ring_wait(2, 1)
    ring_step(3, 1)
    open_group(z)
    open_group(lax.rem(z + Z - 1, Z))
    open_group(lax.rem(z + 1, Z))
    sum_a = la[z].astype(F32)
    sum_b = lb[y].astype(F32)
    for d in NEAR:
        r1a[d].wait_recv()
        sum_a += ra[lax.rem(z + Z - d, Z)].astype(F32)
        r1b[d].wait_recv()
        sum_b += rb[lax.rem(y + Y - d, Y)].astype(F32)
    ra2[y] = sum_a.astype(BF16)
    rb2[z] = sum_b.astype(BF16)
    r2a, r2b = {}, {}
    for d in FAR:
        r2a[d] = send(ra2.at[y], ra2.at[y], r2a_s.at[d], r2a_r.at[d], at_y(d))
        r2b[d] = send(rb2.at[z], rb2.at[z], r2b_s.at[d], r2b_r.at[d], at_z(d))

    ring_wait(3, 0)
    ring_step(4, 0)
    ring_wait(3, 1)
    ring_step(4, 1)
    open_group(lax.rem(z + Z - 2, Z))
    open_group(lax.rem(z + 2, Z))
    open_group(lax.rem(z + Z - 3, Z))
    open_group(lax.rem(z + 3, Z))
    for d in NEAR:
        g1a[d].wait_recv()
        g1b[d].wait_recv()

    def directions(sums, moments, lows):
        low = sums[0].astype(F32)
        for k in range(1, 8):
            low += sums[k].astype(F32)
        lows[...] = low
        moment = 0.8 * moments[:, 0] + 0.2 * low
        spread = 0.95 * moments[:, 1] + 0.05 * low * low
        return encode(moment / (jnp.sqrt(spread) + 1e-08), DIRECTION_RATE)

    g2a, g2b = {}, {}
    for d in NEAR:
        r2a[d].wait_recv()
    da[z] = directions(ra2, ma, sa)
    for d in FAR:
        g2a[d] = send(da.at[z], da.at[z], g2a_s.at[d], g2a_r.at[d], at_z(d))
    for d in NEAR:
        r2b[d].wait_recv()
    db[y] = directions(rb2, mb, sb)
    for d in FAR:
        g2b[d] = send(db.at[y], db.at[y], g2b_s.at[d], g2b_r.at[d], at_y(d))
    low_v[...] = jnp.concatenate([sa[y], sb[z]], axis=1)

    ring_wait(4, 0)
    ring_wait(4, 1)
    open_group(lax.rem(z + 4, Z))
    for k in range(Z):
        wo_f[:, k * 256 : (k + 1) * 256] = decode(wo[k].reshape(256, 256).T, WEIGHT_RATE)
    for d in NEAR:
        g2a[d].wait_recv()
        g2b[d].wait_recv()
    sent = to_pair + passed
    for group in (w1v, w1o, x_sum, x_all, r1a, r1b, r2a, r2b, g1a, g1b, g2a, g2b):
        sent += list(group.values())
    for ring in rings.values():
        sent += ring
    for copy in sent:
        copy.wait_send()


def finish_kernel(
    da, db, wv, wo, low, vf, of, vw, ow, vm, vs, om, os_,
    vmaster, omaster, vm_new, vs_new, om_new, os_new, vcopy, ocopy,
    dv, do, do_t, vc_v, oc_v, n_v, k_v, out_sem, chunk_sem,
):
    fs = lax.axis_index("fs")
    upper = lax.broadcasted_iota(jnp.int32, (8, 256), 0) < 4
    for g in range(Z * Y // 2):
        zz, yy = (2 * g) // Y, (2 * g) % Y
        even = jnp.concatenate([da[zz, yy], db[yy, zz]], axis=1)
        odd = jnp.concatenate([da[zz, yy + 1], db[yy + 1, zz]], axis=1)
        even = 0.05 * decode(even, DIRECTION_RATE)
        odd = 0.05 * decode(odd, DIRECTION_RATE)
        value = jnp.where(upper, even, pltpu.roll(odd, 4, 0))
        output = jnp.where(upper, pltpu.roll(even, 4, 0), odd)
        for full, both in ((value, dv), (output, do)):
            top = full.astype(BF16)
            both[8 * g : 8 * g + 8] = top
            both[RANK + 8 * g : RANK + 8 * g + 8] = (full - top.astype(F32)).astype(BF16)
    do_t[...] = do[...].T
    outs = []

    def put(src, dst, sem):
        copy = pltpu.make_async_copy(src, dst, sem)
        copy.start()
        outs.append(copy)

    for k in range(CHUNKS):
        rows = pl.ds(k * STEP, STEP)
        factor = vf[rows]
        step = jnp.dot(
            jnp.concatenate([factor, factor], axis=1), dv[...], preferred_element_type=F32
        )
        vc_v[rows] = (wv[rows] - step).astype(BF16)
        put(vc_v.at[rows], vcopy.at[rows], chunk_sem.at[k])
    for k in range(CHUNKS):
        rows = pl.ds(k * STEP, STEP)
        factor = of[rows]
        step = lax.dot_general(
            do_t[...],
            jnp.concatenate([factor, factor], axis=1),
            (((1,), (1,)), ((), ())),
            preferred_element_type=F32,
        )
        oc_v[:, rows] = (wo[:, rows] - step).astype(BF16)
        put(oc_v.at[:, rows], ocopy.at[:, rows], chunk_sem.at[CHUNKS + k])
        if k == 0:
            low_v, low_o = low[0:4], low[4:8]
            n_v[0] = 0.8 * vm[...] + 0.2 * low_v
            n_v[1] = 0.95 * vs[...] + 0.05 * low_v * low_v
            n_v[2] = 0.8 * om[...] + 0.2 * low_o
            n_v[3] = 0.95 * os_[...] + 0.05 * low_o * low_o
            for i, dst in enumerate((vm_new, vs_new, om_new, os_new)):
                put(n_v.at[i], dst, out_sem.at[i])
    own = pl.ds(pl.multiple_of(fs * WIDTH_ROWS, WIDTH_ROWS), WIDTH_ROWS)
    for i, (factor, both, weight, out) in enumerate(
        ((vf, dv, vw, vmaster), (of, do, ow, omaster))
    ):
        rows = factor[own]
        k_v[i] = weight[...] - jnp.dot(
            jnp.concatenate([rows, rows], axis=1), both[...], preferred_element_type=F32
        )
        put(k_v.at[i], out, out_sem.at[4 + i])
    for copy in outs:
        copy.wait()


def local(
    inputs, value_cotangent, first_map, second_map, lambdas, head_gain, output_cotangent,
    value_factor, output_factor, value_weight, output_weight,
    value_moment, value_second, output_moment, output_second,
):
    turned_weight = output_weight.T
    gain = head_gain.reshape(1, HEAD)
    hbm = pl.BlockSpec(memory_space=pltpu.HBM)
    near = pl.BlockSpec(memory_space=pltpu.VMEM)
    dma = pltpu.SemaphoreType.DMA
    vmem = pltpu.VMEM
    sems = [dma((17,)), dma((2,)), dma((2,))] + [dma((8,))] * 6
    sems += [dma((8,))] * 20 + [dma((16,))] * 4
    far = [
        pltpu.with_memory_space_constraint(a, pltpu.HBM)
        for a in (
            inputs, output_cotangent, value_cotangent, first_map, second_map, lambdas, gain,
            value_factor, output_factor, value_weight, turned_weight,
            value_moment, value_second, output_moment, output_second,
        )
    ]
    wv, wo, da, db, low = pl.pallas_call(
        exchange_kernel,
        out_shape=[
            jax.ShapeDtypeStruct((Z, 256, 256), F32),
            jax.ShapeDtypeStruct((256, 2048), F32),
            jax.ShapeDtypeStruct((Z, Y, 8, 128), BF16),
            jax.ShapeDtypeStruct((Y, Z, 8, 128), BF16),
            jax.ShapeDtypeStruct((8, 256), F32),
        ],
        in_specs=[hbm] * 5
        + [pl.BlockSpec(memory_space=pltpu.SMEM), pl.BlockSpec(memory_space=pltpu.VMEM)]
        + [hbm] * 8,
        out_specs=[near] * 5,
        scratch_shapes=[
            vmem((512, 256), BF16), vmem((512, 256), BF16), vmem((512, 256), BF16),
            vmem((512, 256), BF16), vmem((512, 256), BF16),
            vmem((512, 256), BF16), vmem((512, 256), BF16),
            vmem((WIDTH_ROWS, 256), F32), vmem((WIDTH_ROWS, 256), F32),
            vmem((Y, 2, 8, 128), F32), vmem((Z, 2, 8, 128), F32),
            vmem((2, 256, 256), BF16), vmem((2, X, 32, 512), F32), vmem((2, X, 32, 512), BF16),
            vmem((2, X, 32, 512), BF16), vmem((C, X, 2, 32, 512), BF16), vmem((512, 256), BF16),
            vmem((Z, Y, 8, 128), BF16), vmem((Y, Z, 8, 128), BF16),
            vmem((Z, Y, 8, 128), BF16), vmem((Y, Z, 8, 128), BF16),
            vmem((Y, 8, 128), F32), vmem((Z, 8, 128), F32),
            vmem((Y, Y, 8, 128), BF16), vmem((Z, Z, 8, 128), BF16),
            vmem((Z, Y, WIDTH_ROWS, 256), BF16), vmem((Z, Y, WIDTH_ROWS, 256), BF16),
        ]
        + sems,
        compiler_params=pltpu.CompilerParams(
            collective_id=0, has_side_effects=True, vmem_limit_bytes=24 * 1024 * 1024
        ),
        name="exchange",
    )(*far)
    width, cols = 2048, 256
    wv = wv.reshape(width, cols)

    small = jax.ShapeDtypeStruct((4, cols), F32)
    own = jax.ShapeDtypeStruct((WIDTH_ROWS, cols), F32)
    vmaster, omaster, *rest = pl.pallas_call(
        finish_kernel,
        out_shape=[
            own, own, small, small, small, small,
            jax.ShapeDtypeStruct((width, cols), BF16),
            jax.ShapeDtypeStruct((cols, width), BF16),
        ],
        in_specs=[near] * 13,
        out_specs=[hbm] * 8,
        scratch_shapes=[
            vmem((2 * RANK, cols), BF16), vmem((2 * RANK, cols), BF16), vmem((cols, 2 * RANK), BF16),
            vmem((width, cols), BF16), vmem((cols, width), BF16),
            vmem((4, 4, cols), F32), vmem((2, WIDTH_ROWS, cols), F32),
            dma((6,)), dma((2 * CHUNKS,)),
        ],
        compiler_params=pltpu.CompilerParams(vmem_limit_bytes=24 * 1024 * 1024),
        name="finish",
    )(
        da, db, wv, wo, low, value_factor, output_factor, value_weight, turned_weight,
        value_moment, value_second, output_moment, output_second,
    )
    return (vmaster, omaster.T, *rest)


def solution(mesh):
    both = P("fs", "tp")
    in_specs = (
        both, both, both, both, P("tp"), P(), both, P(), P(), both, P("tp", "fs"),
        both, both, both, both,
    )
    out_specs = (
        both, P("tp", "fs"), both, both, both, both, P(None, "tp"), P("tp", None),
    )
    return jax.shard_map(local, mesh=mesh, in_specs=in_specs, out_specs=out_specs, check_vma=False)
```

```python
import functools
import math

import jax
import jax.numpy as jnp
from jax import lax
from jax.experimental import pallas as pl
from jax.experimental.pallas import tpu as pltpu
from jax.sharding import PartitionSpec as P

MESH = pl.DeviceIdType.MESH
X, C, Y, Z = 4, 2, 8, 8
F32, BF16 = jnp.float32, jnp.bfloat16
RANK, HEAD = 256, 128
FAR = (4, 3, 5, 2, 6, 1, 7)
NEAR = (1, 7, 2, 6, 3, 5, 4)
WIDTH_ROWS = 32
STEP = 512
CHUNKS = 2048 // STEP
WEIGHT_RATE = 960.0
DIRECTION_RATE = 11.0


def encode(value, rate):
    size = jnp.exp2(jnp.abs(value) * rate) - 1.0
    return jnp.where(value < 0, -size, size).astype(BF16)


def decode(code, rate):
    code = code.astype(F32)
    size = jnp.log(1.0 + jnp.abs(code)) * (1.0 / (rate * math.log(2.0)))
    return jnp.where(code < 0, -size, size)


def rows_dot(left, right):
    return lax.dot_general(left, right, (((0,), (0,)), ((), ())), preferred_element_type=F32)


def exchange_kernel(
    inputs, ocot, vcot, first, second, lambdas, gain, vf, of, vw, ow, vm, vs, om, os_,
    wv_f, wo_f, da, db, low_v,
    in_v, oc_v, vc_v, fi_v, se_v, vf_v, of_v, vw_v, ow_v, la_v, ga_v, ma, mb,
    pair, ax, sx, rx, pq, heads,
    la, lb, ra, rb, sa, sb, ra2, rb2, wv, wo,
    load_sem,
    pair_s, pair_r, xs_s, xs_r, xg_s, xg_r, fw_s, fw_r,
    r1a_s, r1a_r, r1b_s, r1b_r, r2a_s, r2a_r, r2b_s, r2b_r,
    g1a_s, g1a_r, g1b_s, g1b_r, g2a_s, g2a_r, g2b_s, g2b_r,
    w1v_s, w1v_r, w1o_s, w1o_r, wrv_s, wrv_r, wro_s, wro_r,
):
    fs = lax.axis_index("fs")
    tp = lax.axis_index("tp")
    z, y = fs // Y, lax.rem(fs, Y)
    x, c = tp // C, lax.rem(tp, C)

    def at_x(d):
        return (fs, lax.rem(x + d, X) * C + c)

    def at_y(d):
        return (z * Y + lax.rem(y + d, Y), tp)

    def at_z(d):
        return (lax.rem(z + d, Z) * Y + y, tp)

    partner = (fs, x * C + (1 - c))

    def send(src, dst, s, r, where):
        copy = pltpu.make_async_remote_copy(
            src_ref=src, dst_ref=dst, send_sem=s, recv_sem=r, device_id=where, device_id_type=MESH
        )
        copy.start()
        return copy

    barrier = pltpu.get_barrier_semaphore()
    friends = (
        [at_y(d) for d in FAR] + [at_z(d) for d in FAR] + [at_x(d) for d in (2, 1, 3)] + [partner]
    )
    for friend in friends:
        pl.semaphore_signal(barrier, inc=1, device_id=friend, device_id_type=MESH)

    chip_rows = pl.ds(pl.multiple_of(x * (C * 256), C * 256), C * 256)
    loads = {}
    for i, (name, src, dst) in enumerate(
        [
            ("vw", vw, vw_v),
            ("ow", ow, ow_v),
            ("in", inputs, in_v),
            ("vf", vf.at[chip_rows], vf_v),
            ("oc", ocot, oc_v),
            ("of", of.at[chip_rows], of_v),
            ("la", lambdas, la_v),
            ("ga", gain, ga_v),
            ("fi", first, fi_v),
            ("se", second, se_v),
            ("vc", vcot, vc_v),
        ]
        + [
            (f"{name}{i}", src.at[:, pl.ds(i * 128, 128)], dst.at[kind, pl.ds(row, 4)])
            for i, dst in enumerate((ma.at[y], mb.at[z]))
            for name, src, kind, row in (
                ("vm", vm, 0, 0), ("om", om, 0, 4), ("vs", vs, 1, 0), ("os", os_, 1, 4)
            )
        ]
    ):
        loads[name] = pltpu.make_async_copy(src, dst, load_sem.at[i])
        loads[name].start()

    mine = pl.ds(pl.multiple_of(c * 256, 256), 256)
    theirs = pl.ds(pl.multiple_of((1 - c) * 256, 256), 256)
    pl.semaphore_wait(barrier, len(friends))
    to_pair = [
        send(inputs.at[theirs], pair.at[0], pair_s.at[0], pair_r.at[0], partner),
        send(ocot.at[theirs], pair.at[1], pair_s.at[1], pair_r.at[1], partner),
    ]
    loads["vw"].wait()
    wv[z, y] = encode(vw_v[...], WEIGHT_RATE)
    loads["ow"].wait()
    wo[z, y] = encode(ow_v[...], WEIGHT_RATE)
    w1v, w1o = {}, {}
    for d in FAR:
        w1v[d] = send(wv.at[z, y], wv.at[z, y], w1v_s.at[d], w1v_r.at[d], at_y(d))
        w1o[d] = send(wo.at[z, y], wo.at[z, y], w1o_s.at[d], w1o_r.at[d], at_z(d))
    for name in ("in", "vf", "oc", "of"):
        loads[name].wait()
    for copy in to_pair:
        copy.wait_recv()
    x_sum = {}
    for h in range(2):

        def part(tokens):
            return tokens.reshape(X, 64, 256)[:, h * 32 : (h + 1) * 32].reshape(X * 32, 256)

        acc_p = jnp.dot(part(in_v[mine]), vf_v[mine], preferred_element_type=F32)
        acc_q = jnp.dot(part(oc_v[mine]), of_v[mine], preferred_element_type=F32)
        acc_p += jnp.dot(part(pair[0]), vf_v[theirs], preferred_element_type=F32)
        acc_q += jnp.dot(part(pair[1]), of_v[theirs], preferred_element_type=F32)
        acc = jnp.concatenate([acc_p, acc_q], axis=1).reshape(X, 32, 512)
        ax[h] = acc
        sx[h] = acc.astype(BF16)
        for d in (2, 1, 3):
            k = 4 * h + d
            x_sum[h, d] = send(
                sx.at[h, lax.rem(x + d, X)], rx.at[h, x], xs_s.at[k], xs_r.at[k], at_x(d)
            )

    def ring_step(s, h):
        half = pl.ds(h * 4, 4)
        moves = []
        if s < 4 or h == 0:
            zz, yy = lax.rem(z + Z - (s - 1), Z), lax.rem(y + Y - (s - 1), Y)
            k = 4 * (s - 1) + 2 * h
            moves += [(wv.at[zz, half], wrv_s, wrv_r, k, at_z(1))]
            moves += [(wo.at[half, pl.ds(yy, 1)], wro_s, wro_r, k, at_y(1))]
        if s < 4 or h == 1:
            zz, yy = lax.rem(z + (s - 1), Z), lax.rem(y + (s - 1), Y)
            k = 4 * (s - 1) + 2 * h + 1
            moves += [(wv.at[zz, half], wrv_s, wrv_r, k, at_z(Z - 1))]
            moves += [(wo.at[half, pl.ds(yy, 1)], wro_s, wro_r, k, at_y(Y - 1))]
        rings[s, h] = [
            send(ref, ref, ss.at[k], rs.at[k], where) for ref, ss, rs, k, where in moves
        ]

    def ring_wait(s, h):
        for copy in rings[s, h]:
            copy.wait_recv()

    rings = {}

    def open_group(at):
        wv_f[at] = decode(wv[at].reshape(256, 256), WEIGHT_RATE)

    for d in NEAR:
        w1v[d].wait_recv()
        w1o[d].wait_recv()
    for name in ("vm", "om", "vs", "os"):
        loads[name + "0"].wait()
        loads[name + "1"].wait()
    g1a, g1b = {}, {}
    for d in FAR:
        g1a[d] = send(ma.at[y], ma.at[y], g1a_s.at[d], g1a_r.at[d], at_y(d))
        g1b[d] = send(mb.at[z], mb.at[z], g1b_s.at[d], g1b_r.at[d], at_z(d))
    ring_step(1, 0)
    ring_step(1, 1)

    loads["la"].wait()
    loads["ga"].wait()
    loads["fi"].wait()
    loads["se"].wait()
    for h in range(2):
        cols = slice(h * HEAD, (h + 1) * HEAD)
        difference = fi_v[:, cols].astype(F32) - la_v[h] * se_v[:, cols].astype(F32)
        mean = jnp.mean(difference * difference, axis=-1, keepdims=True)
        heads[:, cols] = (difference * lax.rsqrt(mean + 1e-06) * ga_v[...]).astype(BF16)

    x_all, passed = {}, []
    for h in range(2):
        total = ax[h, x]
        for d in (1, 3, 2):
            x_sum[h, d].wait_recv()
            total += rx[h, lax.rem(x + X - d, X)].astype(F32)
        pq[c, x, h] = total.astype(BF16)
        block = pq.at[c, x, h]
        for d in (2, 1, 3):
            k = 4 * h + d
            x_all[h, d] = send(block, block, xg_s.at[k], xg_r.at[k], at_x(d))
        passed.append(send(block, block, fw_s.at[4 * h], fw_r.at[4 * h], partner))

    ring_wait(1, 0)
    ring_step(2, 0)
    ring_wait(1, 1)
    ring_step(2, 1)

    for h in range(2):
        for d in (1, 3, 2):
            x_all[h, d].wait_recv()
            block = pq.at[c, lax.rem(x + X - d, X), h]
            k = 4 * h + d
            passed.append(send(block, block, fw_s.at[k], fw_r.at[k], partner))
    loads["vc"].wait()
    pq_mine = pq[c].reshape(256, 512)
    lv = rows_dot(pq_mine[:, :RANK], vc_v[mine])
    lo = rows_dot(pq_mine[:, RANK:], heads[mine])
    for copy in passed:
        copy.wait_recv()
    pq_theirs = pq[1 - c].reshape(256, 512)
    lv += rows_dot(pq_theirs[:, :RANK], vc_v[theirs])
    lo += rows_dot(pq_theirs[:, RANK:], heads[theirs])
    scale = 1.0 / math.sqrt(32768.0)
    lv3 = (lv * scale).reshape(32, 8, 256)
    lo3 = (lo * scale).reshape(32, 8, 256)
    upper = lax.broadcasted_iota(jnp.int32, (32, 8, 256), 1) < 4
    even = jnp.where(upper, lv3, pltpu.roll(lo3, 4, 1)).astype(BF16)
    odd = jnp.where(upper, pltpu.roll(lv3, 4, 1), lo3).astype(BF16)
    for f in range(Z * Y):
        block = (odd if f % 2 else even)[f // 2]
        la[f // Y, f % Y] = block[:, :128]
        lb[f % Y, f // Y] = block[:, 128:]
    r1a, r1b = {}, {}
    for d in FAR:
        r1a[d] = send(la.at[lax.rem(z + d, Z)], ra.at[z], r1a_s.at[d], r1a_r.at[d], at_z(d))
        r1b[d] = send(lb.at[lax.rem(y + d, Y)], rb.at[y], r1b_s.at[d], r1b_r.at[d], at_y(d))

    ring_wait(2, 0)
    ring_step(3, 0)
    ring_wait(2, 1)
    ring_step(3, 1)
    open_group(z)
    open_group(lax.rem(z + Z - 1, Z))
    open_group(lax.rem(z + 1, Z))
    r2a, r2b = {}, {}
    sum_a = la[z].astype(F32)
    for d in NEAR:
        r1a[d].wait_recv()
        sum_a += ra[lax.rem(z + Z - d, Z)].astype(F32)
    ra2[y] = sum_a.astype(BF16)
    for d in FAR:
        r2a[d] = send(ra2.at[y], ra2.at[y], r2a_s.at[d], r2a_r.at[d], at_y(d))
    sum_b = lb[y].astype(F32)
    for d in NEAR:
        r1b[d].wait_recv()
        sum_b += rb[lax.rem(y + Y - d, Y)].astype(F32)
    rb2[z] = sum_b.astype(BF16)
    for d in FAR:
        r2b[d] = send(rb2.at[z], rb2.at[z], r2b_s.at[d], r2b_r.at[d], at_z(d))

    ring_wait(3, 0)
    ring_step(4, 0)
    ring_wait(3, 1)
    ring_step(4, 1)
    open_group(lax.rem(z + Z - 2, Z))
    open_group(lax.rem(z + 2, Z))
    open_group(lax.rem(z + Z - 3, Z))
    open_group(lax.rem(z + 3, Z))
    for d in NEAR:
        g1a[d].wait_recv()
        g1b[d].wait_recv()

    def directions(sums, moments, lows):
        low = sums[0].astype(F32)
        for k in range(1, 8):
            low += sums[k].astype(F32)
        lows[...] = low
        moment = 0.8 * moments[:, 0] + 0.2 * low
        spread = 0.95 * moments[:, 1] + 0.05 * low * low
        return encode(moment / (jnp.sqrt(spread) + 1e-08), DIRECTION_RATE)

    g2a, g2b = {}, {}
    for d in NEAR:
        r2a[d].wait_recv()
    da[z] = directions(ra2, ma, sa)
    for d in FAR:
        g2a[d] = send(da.at[z], da.at[z], g2a_s.at[d], g2a_r.at[d], at_z(d))
    for d in NEAR:
        r2b[d].wait_recv()
    db[y] = directions(rb2, mb, sb)
    for d in FAR:
        g2b[d] = send(db.at[y], db.at[y], g2b_s.at[d], g2b_r.at[d], at_y(d))
    low_v[...] = jnp.concatenate([sa[y], sb[z]], axis=1)

    ring_wait(4, 0)
    ring_wait(4, 1)
    open_group(lax.rem(z + 4, Z))
    for k in range(Z):
        wo_f[:, k * 256 : (k + 1) * 256] = decode(wo[k].reshape(256, 256).T, WEIGHT_RATE)
    for d in NEAR:
        g2a[d].wait_recv()
        g2b[d].wait_recv()
    sent = to_pair + passed
    for group in (w1v, w1o, x_sum, x_all, r1a, r1b, r2a, r2b, g1a, g1b, g2a, g2b):
        sent += list(group.values())
    for ring in rings.values():
        sent += ring
    for copy in sent:
        copy.wait_send()


def finish_kernel(
    da, db, wv, wo, low, vf, of, vw, ow, vm, vs, om, os_,
    vmaster, omaster, vm_new, vs_new, om_new, os_new, vcopy, ocopy,
    dv, do, do_t, vc_v, oc_v, n_v, k_v, out_sem, chunk_sem,
):
    fs = lax.axis_index("fs")
    upper = lax.broadcasted_iota(jnp.int32, (8, 256), 0) < 4
    for g in range(Z * Y // 2):
        zz, yy = (2 * g) // Y, (2 * g) % Y
        even = jnp.concatenate([da[zz, yy], db[yy, zz]], axis=1)
        odd = jnp.concatenate([da[zz, yy + 1], db[yy + 1, zz]], axis=1)
        even = 0.05 * decode(even, DIRECTION_RATE)
        odd = 0.05 * decode(odd, DIRECTION_RATE)
        value = jnp.where(upper, even, pltpu.roll(odd, 4, 0))
        output = jnp.where(upper, pltpu.roll(even, 4, 0), odd)
        for full, both in ((value, dv), (output, do)):
            top = full.astype(BF16)
            both[8 * g : 8 * g + 8] = top
            both[RANK + 8 * g : RANK + 8 * g + 8] = (full - top.astype(F32)).astype(BF16)
    do_t[...] = do[...].T
    outs = []

    def put(src, dst, sem):
        copy = pltpu.make_async_copy(src, dst, sem)
        copy.start()
        outs.append(copy)

    for k in range(CHUNKS):
        rows = pl.ds(k * STEP, STEP)
        factor = vf[rows]
        step = jnp.dot(
            jnp.concatenate([factor, factor], axis=1), dv[...], preferred_element_type=F32
        )
        vc_v[rows] = (wv[rows] - step).astype(BF16)
        put(vc_v.at[rows], vcopy.at[rows], chunk_sem.at[k])
    for k in range(CHUNKS):
        rows = pl.ds(k * STEP, STEP)
        factor = of[rows]
        step = lax.dot_general(
            do_t[...],
            jnp.concatenate([factor, factor], axis=1),
            (((1,), (1,)), ((), ())),
            preferred_element_type=F32,
        )
        oc_v[:, rows] = (wo[:, rows] - step).astype(BF16)
        put(oc_v.at[:, rows], ocopy.at[:, rows], chunk_sem.at[CHUNKS + k])
        if k == 0:
            low_v, low_o = low[0:4], low[4:8]
            n_v[0] = 0.8 * vm[...] + 0.2 * low_v
            n_v[1] = 0.95 * vs[...] + 0.05 * low_v * low_v
            n_v[2] = 0.8 * om[...] + 0.2 * low_o
            n_v[3] = 0.95 * os_[...] + 0.05 * low_o * low_o
            for i, dst in enumerate((vm_new, vs_new, om_new, os_new)):
                put(n_v.at[i], dst, out_sem.at[i])
    own = pl.ds(pl.multiple_of(fs * WIDTH_ROWS, WIDTH_ROWS), WIDTH_ROWS)
    for i, (factor, both, weight, out) in enumerate(
        ((vf, dv, vw, vmaster), (of, do, ow, omaster))
    ):
        rows = factor[own]
        k_v[i] = weight[...] - jnp.dot(
            jnp.concatenate([rows, rows], axis=1), both[...], preferred_element_type=F32
        )
        put(k_v.at[i], out, out_sem.at[4 + i])
    for copy in outs:
        copy.wait()


def local(
    inputs, value_cotangent, first_map, second_map, lambdas, head_gain, output_cotangent,
    value_factor, output_factor, value_weight, output_weight,
    value_moment, value_second, output_moment, output_second,
):
    turned_weight = output_weight.T
    gain = head_gain.reshape(1, HEAD)
    hbm = pl.BlockSpec(memory_space=pltpu.HBM)
    near = pl.BlockSpec(memory_space=pltpu.VMEM)
    dma = pltpu.SemaphoreType.DMA
    vmem = pltpu.VMEM
    sems = [dma((19,)), dma((2,)), dma((2,))] + [dma((8,))] * 6
    sems += [dma((8,))] * 20 + [dma((16,))] * 4
    far = [
        pltpu.with_memory_space_constraint(a, pltpu.HBM)
        for a in (
            inputs, output_cotangent, value_cotangent, first_map, second_map, lambdas, gain,
            value_factor, output_factor, value_weight, turned_weight,
            value_moment, value_second, output_moment, output_second,
        )
    ]
    wv, wo, da, db, low = pl.pallas_call(
        exchange_kernel,
        out_shape=[
            jax.ShapeDtypeStruct((Z, 256, 256), F32),
            jax.ShapeDtypeStruct((256, 2048), F32),
            jax.ShapeDtypeStruct((Z, Y, 8, 128), BF16),
            jax.ShapeDtypeStruct((Y, Z, 8, 128), BF16),
            jax.ShapeDtypeStruct((8, 256), F32),
        ],
        in_specs=[hbm] * 5
        + [hbm] * 10,
        out_specs=[near] * 5,
        scratch_shapes=[
            vmem((512, 256), BF16), vmem((512, 256), BF16), vmem((512, 256), BF16),
            vmem((512, 256), BF16), vmem((512, 256), BF16),
            vmem((512, 256), BF16), vmem((512, 256), BF16),
            vmem((WIDTH_ROWS, 256), F32), vmem((WIDTH_ROWS, 256), F32),
            pltpu.SMEM((2,), F32), vmem((1, HEAD), F32),
            vmem((Y, 2, 8, 128), F32), vmem((Z, 2, 8, 128), F32),
            vmem((2, 256, 256), BF16), vmem((2, X, 32, 512), F32), vmem((2, X, 32, 512), BF16),
            vmem((2, X, 32, 512), BF16), vmem((C, X, 2, 32, 512), BF16), vmem((512, 256), BF16),
            vmem((Z, Y, 8, 128), BF16), vmem((Y, Z, 8, 128), BF16),
            vmem((Z, Y, 8, 128), BF16), vmem((Y, Z, 8, 128), BF16),
            vmem((Y, 8, 128), F32), vmem((Z, 8, 128), F32),
            vmem((Y, Y, 8, 128), BF16), vmem((Z, Z, 8, 128), BF16),
            vmem((Z, Y, WIDTH_ROWS, 256), BF16), vmem((Z, Y, WIDTH_ROWS, 256), BF16),
        ]
        + sems,
        compiler_params=pltpu.CompilerParams(
            collective_id=0, has_side_effects=True, vmem_limit_bytes=24 * 1024 * 1024
        ),
        name="exchange",
    )(*far)
    width, cols = 2048, 256
    wv = wv.reshape(width, cols)

    small = jax.ShapeDtypeStruct((4, cols), F32)
    own = jax.ShapeDtypeStruct((WIDTH_ROWS, cols), F32)
    vmaster, omaster, *rest = pl.pallas_call(
        finish_kernel,
        out_shape=[
            own, own, small, small, small, small,
            jax.ShapeDtypeStruct((width, cols), BF16),
            jax.ShapeDtypeStruct((cols, width), BF16),
        ],
        in_specs=[near] * 13,
        out_specs=[hbm] * 8,
        scratch_shapes=[
            vmem((2 * RANK, cols), BF16), vmem((2 * RANK, cols), BF16), vmem((cols, 2 * RANK), BF16),
            vmem((width, cols), BF16), vmem((cols, width), BF16),
            vmem((4, 4, cols), F32), vmem((2, WIDTH_ROWS, cols), F32),
            dma((6,)), dma((2 * CHUNKS,)),
        ],
        compiler_params=pltpu.CompilerParams(vmem_limit_bytes=24 * 1024 * 1024),
        name="finish",
    )(
        da, db, wv, wo, low, value_factor, output_factor, value_weight, turned_weight,
        value_moment, value_second, output_moment, output_second,
    )
    return (vmaster, omaster.T, *rest)


def solution(mesh):
    both = P("fs", "tp")
    in_specs = (
        both, both, both, both, P("tp"), P(), both, P(), P(), both, P("tp", "fs"),
        both, both, both, both,
    )
    out_specs = (
        both, P("tp", "fs"), both, both, both, both, P(None, "tp"), P("tp", None),
    )
    return jax.shard_map(local, mesh=mesh, in_specs=in_specs, out_specs=out_specs, check_vma=False)
```
